256 devices in a mesh: sp: 32 (over z, x), tp: 8 (over y, core).
Axes of the slice: x: 4, y: 4, z: 8, core: 2. Of those that a mesh axis runs over, the one named last changes fastest.
Arguments:
- residual: bfloat16 [24576, 2048], P(('sp', 'tp')), may hold values from -6 to 6
- queries: bfloat16 [24576, 1024], P('sp', 'tp'), may hold values from -6 to 6
- key_rows: bfloat16 [24576, 1024], P('sp', 'tp'), may hold values from -6 to 6
- value_rows: bfloat16 [24576, 1024], P('sp', 'tp'), may hold values from -6 to 6
- gate_rows: bfloat16 [24576, 1024], P('sp', 'tp'), may hold values from -6 to 6
- log_decay: float32 [8, 24576], P('tp', 'sp'), may hold values from -1.7 to 0, as said below
- out_gain: float32 [1024], P('tp'), may hold values from 0.1 to 1.9
- out_weight: bfloat16 [1024, 2048], P('tp'), may hold values from -0.1875 to 0.1875
- norm_gain: float32 [2048], replicated, may hold values from 0.1 to 1.9
- expert_gate: bfloat16 [32, 2048, 4096], P('sp', None, 'tp'), may hold values from -0.125 to 0.125
- expert_up: bfloat16 [32, 2048, 4096], P('sp', None, 'tp'), may hold values from -0.125 to 0.125
- expert_down: bfloat16 [32, 4096, 2048], P('sp', 'tp'), may hold values from -0.09375 to 0.09375
- routes: int32 [24576, 2], P(('sp', 'tp')), may hold values from 0 to 31, all different within a row; in each aligned block of 96 rows (0 to 95, 96 to 191, ...) at most 7 rows name the same one
- route_weight: float32 [24576, 2], P(('sp', 'tp')), may hold values from 0.2 to 1
Outputs:
- layer_out: bfloat16 [24576, 2048], P(('sp', 'tp'))
The draws below stay inside these ranges and needn't reach their ends.
Inputs may be any that keep to these rules, and one draw needn't show every extreme that they name: `log_decay`: every entry is negative. `routes`: among the 96 rows of one device no expert is named by more than 7 rows; the experts of one row differ.
All inputs are finite; a program needn't handle non-finite values.
Results may differ from the reference program's by a relative error of at most 0.015.
Values may be sent and summed in bfloat16 or wider, within the bound.
No kernel may reach another device: no remote copies, remote signals or barrier semaphores. Data moves between devices by JAX's collectives and lax.ppermute only.
A program may use at most 128 MiB of HBM per device.

```python
import math
import jax
import jax.numpy as jnp
import numpy as np
from jax import lax

D = 2048
RETENTION_HEADS = 8
HEAD_DIM = 128
FF = 4096
TOPK = 2
TOK_DEV = 768
SEQUENCE_TOKENS = 24576
RW = 1024
ROWS_DEV = 96
EXPERTS = 32
CAP = 7
N_SP = 32
N_TP = 8


def draw_log_decay(key, part):
    key_vectors = jax.random.split(jax.random.fold_in(key, 11), 5)
    fast_share = 0.5
    is_fast = jax.random.uniform(key_vectors[0], (RETENTION_HEADS, 1)) < fast_share
    fast_rate = jnp.exp(jax.random.uniform(key_vectors[1], (RETENTION_HEADS, 1), minval=jnp.log(1.0 / 100.0), maxval=jnp.log(1.0 / 30.0)))
    slow_rate = 0.3 / SEQUENCE_TOKENS
    decay_rate = jnp.where(is_fast, fast_rate, slow_rate)
    decay_factor = jax.random.uniform(key_vectors[2], (RETENTION_HEADS, SEQUENCE_TOKENS // TOK_DEV), minval=1.0, maxval=2.5)
    decay_factor = jnp.repeat(decay_factor, TOK_DEV, axis=1)
    reset_position = jax.random.randint(key_vectors[3], (RETENTION_HEADS, 3, 1), 0, SEQUENCE_TOKENS)
    reset_strength = jax.random.uniform(key_vectors[4], (RETENTION_HEADS, 3, 1), minval=jnp.log(0.6), maxval=jnp.log(0.85))
    position_lookup = jnp.arange(SEQUENCE_TOKENS, dtype=jnp.int32)[None, None, :]
    reset_events = jnp.sum(jnp.where(position_lookup == reset_position, reset_strength, 0.0), axis=1)
    return (-decay_rate * decay_factor + reset_events).astype(jnp.float32)


def block_levels(own_key, dims, shards, smallest, top_value):
    factor_of = 1.0
    for dim, parts in shards:
        steps = jax.random.uniform(jax.random.fold_in(jax.random.fold_in(own_key, 6), dim), (parts,), jnp.float32, smallest / len(shards), top_value / len(shards))
        factor_of = factor_of * jnp.repeat(jnp.exp(steps), dims[dim] // parts).reshape((-1,) + (1,) * (len(dims) - 1 - dim))
    return factor_of


def deal_out(stream_key, own, number, rows, amount, top, most, lean):
    sequence = jax.random.permutation(stream_key, amount)
    crowded, ordinary = shares(amount, rows * top, most, lean, True), shares(amount, rows * top, most, lean, False)
    places = jnp.arange(amount)

    def named(lengths, rotation):
        used = int((lengths > 0).sum())
        fixed = max(1, used // 4)
        passed = fixed + (places - fixed + rotation * (used - fixed)) % max(1, amount - fixed)
        return jnp.zeros((amount,), jnp.int32).at[sequence[jnp.where(places < fixed, places, passed)]].set(jnp.asarray(lengths, jnp.int32))

    lengths = jnp.where(number % 4 == 0, named(crowded, number // 4), named(ordinary, number - number // 4 - 1))
    mixed = jax.random.permutation(jax.random.fold_in(own, 3), amount)
    giver, sink = mixed[0:amount // 2 * 2:2], mixed[1:amount // 2 * 2:2]
    slack = jnp.minimum(lengths[giver] - 1, most - lengths[sink]) // 2
    slack = jnp.where((giver == sequence[0]) | (sink == sequence[0]) | (lengths[sink] == 0), 0, jnp.maximum(slack, 0))
    passed = jax.random.randint(jax.random.fold_in(own, 4), (amount // 2,), 0, 1 << 20) % (slack + 1)
    lengths = lengths.at[giver].add(-passed).at[sink].add(passed)
    items = jnp.searchsorted(jnp.cumsum(lengths), jnp.arange(rows * top), side="right").astype(jnp.int32)
    grid = items.reshape(top, rows).T
    grid = grid[jax.random.permutation(jax.random.fold_in(own, 1), rows)]
    rotation = jax.random.randint(jax.random.fold_in(own, 2), (rows, 1), 0, top)
    return jnp.take_along_axis(grid, (jnp.arange(top)[None, :] + rotation) % top, axis=1)


def shares(count, total, limit, lean, full):
    portions = [(1 << 20) // math.isqrt(rank ** lean) + 1 for rank in range(1, count + 1)]
    largest = limit if full else min(limit, max(-(-total // count), total * portions[0] // sum(portions)))
    least = 1 if total - largest >= count - 1 else 0
    given, rest = [largest] + [least] * (count - 1), total - largest - least * (count - 1)
    while rest > 0:
        movable = [i for i in range(1, count) if given[i] < largest] or [i for i in range(1, count) if given[i] < limit]
        whole, left = sum([portions[i] for i in movable]), rest
        for i in movable:
            more = min(limit - given[i], max(1, left * portions[i] // whole), rest)
            given[i] = given[i] + more
            rest = rest - more
    return np.array(given)


def centred(rng, shape, scale, limit, cuts=(), kind=jnp.bfloat16):
    factor_of = block_levels(rng, shape, cuts, -0.22, 0.18) if cuts else 1.0
    values = jax.random.normal(rng, shape, jnp.float32) * scale * factor_of
    return jnp.minimum(jnp.maximum(values, -limit), limit).astype(kind)


def setup_inputs(seed: int = 0) -> dict:
    seeds = jax.random.split(jax.random.key(seed), 15)
    residual = centred(seeds[0], (SEQUENCE_TOKENS, D), 1.0, 6.0, ((0, 256),))
    queries = centred(seeds[1], (SEQUENCE_TOKENS, RW), 1.0, 6.0, ((0, 32), (1, 8)))
    key_rows = centred(seeds[2], (SEQUENCE_TOKENS, RW), 1.0, 6.0, ((0, 32), (1, 8)))
    value_rows = centred(seeds[3], (SEQUENCE_TOKENS, RW), 1.0, 6.0, ((0, 32), (1, 8)))
    gate_rows = centred(seeds[4], (SEQUENCE_TOKENS, RW), 1.0, 6.0, ((0, 32), (1, 8)))
    log_decay = draw_log_decay(jax.random.fold_in(seeds[14], 71), 0)
    out_gain = jnp.clip(1.0 + 0.18 * jax.random.normal(seeds[6], (RW,), jnp.float32), 0.1, 1.9)
    out_weight = centred(seeds[7], (RW, D), RW ** -0.5, 0.1875, ((0, 8),))
    norm_gain = jnp.clip(1.0 + 0.18 * jax.random.normal(seeds[8], (D,), jnp.float32), 0.1, 1.9)
    expert_gate = centred(seeds[9], (EXPERTS, D, FF), D ** -0.5, 0.125, ((0, 32), (2, 8)))
    expert_up = centred(seeds[10], (EXPERTS, D, FF), D ** -0.5, 0.125, ((0, 32), (2, 8)))
    expert_down = centred(seeds[11], (EXPERTS, FF, D), FF ** -0.5, 0.09375, ((0, 32), (1, 8)))
    routes_keys = jax.random.split(jax.random.fold_in(seeds[12], 1), SEQUENCE_TOKENS // ROWS_DEV)
    routes_turns = jax.random.permutation(jax.random.fold_in(seeds[12], 3), SEQUENCE_TOKENS // ROWS_DEV)
    routes = jax.vmap(lambda own, number: deal_out(jax.random.fold_in(seeds[12], 2), own, number, ROWS_DEV, EXPERTS, TOPK, CAP, 2))(routes_keys, routes_turns).reshape((SEQUENCE_TOKENS, TOPK))
    route_weight = jnp.clip(0.2 + 0.8 * jax.random.uniform(seeds[13], (SEQUENCE_TOKENS, TOPK), jnp.float32) ** block_levels(seeds[13], (SEQUENCE_TOKENS, TOPK), ((0, 256),), -0.2, 0.2), 0.2, 1.0)
    return dict(residual=residual, queries=queries, key_rows=key_rows, value_rows=value_rows, gate_rows=gate_rows, log_decay=log_decay, out_gain=out_gain, out_weight=out_weight, norm_gain=norm_gain, expert_gate=expert_gate, expert_up=expert_up, expert_down=expert_down, routes=routes, route_weight=route_weight)


epsilon = 1e-06
rope_base = 10000.0

def rotate(features, positions):
    half_dim = features.shape[-1] // 2
    inverse = rope_base ** (-jnp.arange(0, 2 * half_dim, 2, dtype=jnp.float32) / (2 * half_dim))
    angles = positions[:, None, None] * inverse[None, None, :]
    cosine = jnp.cos(angles)
    sine_part = jnp.sin(angles)
    first_half = features[..., :half_dim]
    second_half = features[..., half_dim:]
    return jnp.concatenate([first_half * cosine - second_half * sine_part, first_half * sine_part + second_half * cosine], axis=-1)

def reference(residual, queries, key_rows, value_rows, gate_rows, log_decay, out_gain, out_weight, norm_gain, expert_gate, expert_up, expert_down, routes, route_weight):
    positions = jnp.arange(SEQUENCE_TOKENS, dtype=jnp.int32).astype(jnp.float32)
    rotated_queries = (rotate(queries.reshape(SEQUENCE_TOKENS, RETENTION_HEADS, HEAD_DIM).astype(jnp.float32), positions) * HEAD_DIM ** (-0.5)).astype(jnp.bfloat16)
    rotated_keys = rotate(key_rows.reshape(SEQUENCE_TOKENS, RETENTION_HEADS, HEAD_DIM).astype(jnp.float32), positions).astype(jnp.bfloat16)
    value_vectors = value_rows.reshape(SEQUENCE_TOKENS, RETENTION_HEADS, HEAD_DIM)
    block_count = SEQUENCE_TOKENS // TOK_DEV
    causal = jnp.arange(TOK_DEV)[:, None] >= jnp.arange(TOK_DEV)[None, :]

    def advance(carry_state, inputs):
        query_block, key_block, value_block, block_decay = inputs
        cumulative = jnp.cumsum(block_decay, axis=1)
        score_matrix = jnp.einsum('vbq,pbq->bvp', query_block.astype(jnp.float32), key_block.astype(jnp.float32))
        spread = cumulative[:, :, None] - cumulative[:, None, :]
        decays = jnp.where(causal[None], jnp.exp(jnp.where(causal[None], spread, 0.0)), 0.0)
        mixed_weights = (score_matrix * decays).astype(jnp.bfloat16)
        within = jnp.einsum('hlm,mhe->lhe', mixed_weights.astype(jnp.float32), value_block.astype(jnp.float32))
        totals = cumulative[:, -1]
        damped_keys = (key_block.astype(jnp.float32) * jnp.exp(totals[None, :] - cumulative.T)[:, :, None]).astype(jnp.bfloat16)
        block_state = jnp.einsum('vrs,vrx->rsx', damped_keys.astype(jnp.float32), value_block.astype(jnp.float32))
        readout = jnp.einsum('lhd,hde->lhe', query_block.astype(jnp.float32), carry_state, precision=lax.Precision.HIGHEST)
        output = within + jnp.exp(cumulative.T)[:, :, None] * readout
        new_state = jnp.exp(totals)[:, None, None] * carry_state + block_state
        return (new_state, output)
    inputs = (rotated_queries.reshape(block_count, TOK_DEV, RETENTION_HEADS, HEAD_DIM), rotated_keys.reshape(block_count, TOK_DEV, RETENTION_HEADS, HEAD_DIM), value_vectors.reshape(block_count, TOK_DEV, RETENTION_HEADS, HEAD_DIM), jnp.transpose(log_decay.reshape(RETENTION_HEADS, block_count, TOK_DEV), (1, 0, 2)))
    start_state = jnp.zeros((RETENTION_HEADS, HEAD_DIM, HEAD_DIM), jnp.float32)
    unused_state, outputs = lax.scan(advance, start_state, inputs)
    head_out = outputs.reshape(SEQUENCE_TOKENS, RETENTION_HEADS, HEAD_DIM)
    head_norm = head_out * lax.rsqrt(lax.optimization_barrier(jnp.mean(head_out * head_out, axis=-1, keepdims=True)) + epsilon)
    mixed = (head_norm.reshape(SEQUENCE_TOKENS, RW) * out_gain[None, :] * jax.nn.silu(gate_rows.astype(jnp.float32))).astype(jnp.bfloat16)
    projected = jnp.dot(mixed, out_weight, preferred_element_type=jnp.float32)
    hidden_res = (residual.astype(jnp.float32) + projected).astype(jnp.bfloat16)
    hidden_f = hidden_res.astype(jnp.float32)
    normed = (hidden_f * lax.rsqrt(lax.optimization_barrier(jnp.mean(hidden_f * hidden_f, axis=-1, keepdims=True)) + epsilon) * norm_gain[None, :]).astype(jnp.bfloat16)
    flat_ids = routes.reshape(-1).astype(jnp.int32)
    order = jnp.argsort(flat_ids, stable=True).astype(jnp.int32)
    counts = lax.optimization_barrier(jnp.sum((flat_ids[:, None] == jnp.arange(EXPERTS, dtype=jnp.int32)[None, :]).astype(jnp.int32), axis=0))
    starts = (jnp.cumsum(counts) - counts).astype(jnp.int32)
    most_rows = N_SP * N_TP * CAP
    padded = jnp.concatenate([order, jnp.zeros((most_rows,), jnp.int32)])
    member_width = FF // N_TP

    def run_expert(index):
        picks = lax.dynamic_slice(padded, (starts[index],), (most_rows,))
        features = jnp.take(normed, picks // TOPK, axis=0)
        gate_part = jnp.dot(features, expert_gate[index], preferred_element_type=jnp.float32)
        up_part = jnp.dot(features, expert_up[index], preferred_element_type=jnp.float32)
        hidden = (jax.nn.silu(gate_part) * up_part).astype(jnp.bfloat16)
        down_here = expert_down[index]
        summed = jnp.zeros((most_rows, D), jnp.float32)
        for member in range(N_TP):
            piece = jnp.dot(hidden[:, member * member_width:(member + 1) * member_width], down_here[member * member_width:(member + 1) * member_width], preferred_element_type=jnp.float32).astype(jnp.bfloat16)
            summed = summed + piece.astype(jnp.float32)
        valid = jnp.arange(most_rows, dtype=jnp.int32) < counts[index]
        return (summed.astype(jnp.bfloat16), jnp.where(valid, picks, SEQUENCE_TOKENS * TOPK).astype(jnp.int32))
    results, targets = lax.map(run_expert, jnp.arange(EXPERTS, dtype=jnp.int32))
    flat_out = jnp.zeros((SEQUENCE_TOKENS * TOPK, D), jnp.bfloat16).at[targets.reshape(-1)].set(results.reshape(-1, D), mode='drop')
    picked = flat_out.reshape(SEQUENCE_TOKENS, TOPK, D).astype(jnp.float32)
    combined = lax.optimization_barrier(jnp.sum(route_weight[:, :, None] * picked, axis=1))
    return (hidden_f + combined).astype(jnp.bfloat16)
```

```python
import jax
import jax.numpy as jnp
from jax import lax
from jax.experimental import pallas as pl
from jax.experimental.pallas import tpu as pltpu
from jax.sharding import Mesh
from jax.sharding import PartitionSpec as P

SP = ("sp_0", "sp_1")
SP_TP = ("sp_0", "sp_1", "tp")


epsilon = 1e-06
rope_base = 10000.0
BF = jnp.bfloat16
F32 = jnp.float32

OTHER_CORE = [(i, i ^ 1) for i in range(8)]
UP = [(i, (i + 2) % 8) for i in range(8)]
DOWN = [(i, (i - 2) % 8) for i in range(8)]
ACROSS = [(i, (i + 4) % 8) for i in range(8)]

SLOTS = 8
USED = 7
TAIL = 256


def dot(a, b):
    return jnp.dot(a, b, preferred_element_type=F32)


def vmem_call(kernel, out_shape, limit=32 * 1024 * 1024, **kwargs):
    return pl.pallas_call(
        kernel,
        out_shape=out_shape,
        compiler_params=pltpu.CompilerParams(vmem_limit_bytes=limit),
        **kwargs,
    )


def onehot(mask):
    return jnp.where(mask, 1.0, 0.0).astype(BF)


def pack_tokens_kernel(x_ref, slot_ref, out_ref):
    rows = lax.broadcasted_iota(jnp.int32, (out_ref.shape[0], x_ref.shape[0]), 0)
    first, second = slot_ref[0:1, :], slot_ref[1:2, :]
    place = rows & 7
    main_row = jnp.where(place < USED, rows, -1)
    main = onehot((main_row == first) | (main_row == second))
    tail_x = x_ref[:, USED * TAIL :]
    for r in range(USED):
        tail_row = jnp.where(place == USED, rows - USED + r, -1)
        tail = onehot((tail_row == first) | (tail_row == second))
        columns = slice(r * TAIL, (r + 1) * TAIL)
        out_ref[:, columns] = (dot(main, x_ref[:, columns]) + dot(tail, tail_x)).astype(BF)


def unpack_rows_kernel(in_ref, low_ref, high_ref):
    half = low_ref.shape[0]
    senders = in_ref.shape[0] // SLOTS
    for k, ref in enumerate((low_ref, high_ref)):
        p = lax.broadcasted_iota(jnp.int32, (half, in_ref.shape[0]), 0) + k * half
        q = lax.broadcasted_iota(jnp.int32, (half, in_ref.shape[0]), 1)
        chosen = onehot(q == (p & (senders - 1)) * SLOTS + p // senders)
        for r in range(USED):
            columns = slice(r * TAIL, (r + 1) * TAIL)
            ref[:, columns] = dot(chosen, in_ref[:, columns]).astype(BF)
        total = jnp.zeros((half, TAIL), F32)
        for r in range(USED):
            if (r + 1) * senders <= k * half or r * senders >= (k + 1) * half:
                continue
            tails = onehot((q == (p & (senders - 1)) * SLOTS + USED) & (p // senders == r))
            total = total + dot(tails, in_ref[:, r * TAIL : (r + 1) * TAIL])
        ref[:, USED * TAIL :] = total.astype(BF)


def repack_rows_kernel(*refs):
    out_ref = refs[-1]
    parts = refs[:-1]
    half = parts[0].shape[0]
    senders = out_ref.shape[0] // SLOTS
    count = len(parts) // 2
    q = lax.broadcasted_iota(jnp.int32, (out_ref.shape[0], half), 0)
    p = lax.broadcasted_iota(jnp.int32, (out_ref.shape[0], half), 1)
    place, sender = q & 7, q // SLOTS

    def summed(k, columns):
        total = parts[k * count][:, columns].astype(F32)
        for ref in parts[k * count + 1 : (k + 1) * count]:
            total = total + ref[:, columns].astype(F32)
        return total.astype(BF)

    main = [onehot((p + k * half == place * senders + sender) & (place < USED)) for k in (0, 1)]
    tail_rows = [summed(k, slice(USED * TAIL, None)) for k in (0, 1)]
    for r in range(USED):
        columns = slice(r * TAIL, (r + 1) * TAIL)
        total = jnp.zeros((out_ref.shape[0], TAIL), F32)
        for k in (0, 1):
            total = total + dot(main[k], summed(k, columns))
            if (r + 1) * senders <= k * half or r * senders >= (k + 1) * half:
                continue
            tail = onehot((p + k * half == r * senders + sender) & (place == USED))
            total = total + dot(tail, tail_rows[k])
        out_ref[:, columns] = total.astype(BF)


def combine_kernel(rows_ref, hidden_ref, slot_ref, weight_ref, out_ref):
    tokens = hidden_ref.shape[0]
    q = lax.broadcasted_iota(jnp.int32, (tokens, rows_ref.shape[0]), 1)

    def split(w):
        high = w.astype(BF)
        return high, (w - high.astype(F32)).astype(BF)

    pairs = [(slot_ref[:, k : k + 1], weight_ref[:, k : k + 1]) for k in (0, 1)]
    high, low = split(sum(jnp.where(q == s, w, 0.0) for s, w in pairs))
    tail = jnp.zeros((tokens, TAIL), F32)
    for r in range(USED):
        columns = slice(r * TAIL, (r + 1) * TAIL)
        rows = rows_ref[:, columns]
        got = dot(high, rows) + dot(low, rows)
        out_ref[:, columns] = (hidden_ref[:, columns].astype(F32) + got).astype(BF)
        tail_high, tail_low = split(
            sum(jnp.where((q == s - r + USED) & ((s & 7) == r), w, 0.0) for s, w in pairs)
        )
        tail = tail + dot(tail_high, rows) + dot(tail_low, rows)
    columns = slice(USED * TAIL, None)
    out_ref[:, columns] = (hidden_ref[:, columns].astype(F32) + tail).astype(BF)


def expert_kernel(*refs, count):
    parts = refs[:count]
    gate_ref, up_ref, down_ref = refs[count : count + 3]
    outs = refs[count + 3 : 2 * count + 3]
    rows, total = refs[2 * count + 3 :]
    step = pl.program_id(0)
    height = parts[0].shape[0]

    @pl.when(step == 0)
    def _():
        for k, part in enumerate(parts):
            rows[k * height : (k + 1) * height, :] = part[...]

    x = rows[...]
    hidden = (jax.nn.silu(dot(x, gate_ref[0])) * dot(x, up_ref[0])).astype(BF)
    piece = dot(hidden, down_ref[0])

    @pl.when(step == 0)
    def _():
        total[...] = piece

    @pl.when(step == pl.num_programs(0) - 1)
    def _():
        value = (total[...] + piece).astype(BF)
        for k, out in enumerate(outs):
            out[...] = value[k * height : (k + 1) * height, :]


def expert(parts, gate, up, down):
    count = len(parts)
    height, width = parts[0].shape
    chunk = gate.shape[2] // 2
    part_spec = pl.BlockSpec((height, width), lambda j: (0, 0))
    return pl.pallas_call(
        lambda *refs: expert_kernel(*refs, count=count),
        grid=(2,),
        in_specs=[part_spec] * count
        + [
            pl.BlockSpec((1, width, chunk), lambda j: (0, 0, j)),
            pl.BlockSpec((1, width, chunk), lambda j: (0, 0, j)),
            pl.BlockSpec((1, chunk, width), lambda j: (0, j, 0)),
        ],
        out_specs=[part_spec] * count,
        out_shape=[jax.ShapeDtypeStruct((height, width), BF)] * count,
        scratch_shapes=[
            pltpu.VMEM((count * height, width), BF),
            pltpu.VMEM((count * height, width), F32),
        ],
        compiler_params=pltpu.CompilerParams(
            dimension_semantics=("arbitrary",), vmem_limit_bytes=40 * 1024 * 1024
        ),
        cost_estimate=pl.CostEstimate(
            flops=6 * count * height * width * gate.shape[2],
            bytes_accessed=2 * (2 * count * height * width + 3 * width * gate.shape[2]),
            transcendentals=count * height * gate.shape[2],
        ),
    )(*parts, gate, up, down)


def shift(a, where):
    return lax.ppermute(a, "tp", where)


def add(*parts):
    return sum(part.astype(F32) for part in parts).astype(BF)


def routed_experts(low, high, gate, up, down):
    below_low, above_high = shift(low, UP), shift(high, DOWN)
    other_low, other_high = shift(low, OTHER_CORE), shift(high, OTHER_CORE)
    below_high, above_low = shift(high, UP), shift(low, DOWN)
    far_low, far_high = shift(below_low, UP), shift(above_high, DOWN)

    def both_cores(a, b):
        outs = expert((a, b, shift(a, OTHER_CORE), shift(b, OTHER_CORE)), gate, up, down)
        return outs[0], outs[1], shift(outs[2], OTHER_CORE), shift(outs[3], OTHER_CORE)

    own = expert((low, high, other_low, other_high), gate, up, down)
    below = both_cores(below_low, below_high)
    above = both_cores(above_low, above_high)
    far = both_cores(far_low, far_high)
    to_above_low = shift(add(far[0], far[2]), UP)
    to_below_high = shift(add(far[1], far[3]), DOWN)
    from_below_high = shift(add(above[1], above[3]), UP)
    from_above_low = shift(add(below[0], below[2]), DOWN)
    from_below_low = shift(add(above[0], above[2], to_above_low), UP)
    from_above_high = shift(add(below[1], below[3], to_below_high), DOWN)
    return (
        (own[0], shift(own[2], OTHER_CORE), from_below_low, from_above_low),
        (own[1], shift(own[3], OTHER_CORE), from_below_high, from_above_high),
    )


def spread_state(total, state, axis):
    high = lax.reduce_precision(total, 8, 7)
    line = jnp.stack([high, total - high]).astype(BF)[:, None]
    line = jnp.pad(jnp.broadcast_to(line, (2, state.shape[1])), ((0, 6), (0, 0)))
    message = jnp.concatenate([state.astype(BF), line])
    count = lax.axis_size(axis)
    pieces = lax.all_to_all(
        jnp.broadcast_to(message[None], (count, *message.shape)), axis, 0, 0, tiled=True
    )
    lines = pieces[:, state.shape[0] : state.shape[0] + 2, 0].astype(F32)
    return lines[:, 0] + lines[:, 1], pieces[:, : state.shape[0]].astype(F32)


def weighted(totals, states, end):
    k = jnp.arange(totals.shape[0])
    between = (k[None, :] > k[:, None]) & (k[None, :] < end)
    weight = jnp.exp(jnp.sum(jnp.where(between, totals[None, :], 0.0), axis=1))
    weight = jnp.where(k < end, weight, 0.0)
    return jnp.sum(weight[:, None, None] * states, axis=0)


def carried_in(total, state):
    totals, states = spread_state(total, state, "sp_1")
    x = lax.axis_index("sp_1")
    inside = weighted(totals, states, x)
    ahead = jnp.sum(jnp.where(jnp.arange(totals.shape[0]) < x, totals, 0.0))
    totals, states = spread_state(
        jnp.sum(totals), weighted(totals, states, totals.shape[0]), "sp_0"
    )
    before = weighted(totals, states, lax.axis_index("sp_0"))
    return jnp.exp(ahead) * before + inside


def rotate(features, cosine, sine):
    half = features.shape[-1] // 2
    a, b = features[:, :half], features[:, half:]
    return jnp.concatenate([a * cosine - b * sine, a * sine + b * cosine], axis=-1)


def slot_indices(route_ids, experts):
    flat_ids = route_ids.reshape(-1)
    chosen = (flat_ids[:, None] == jnp.arange(experts, dtype=jnp.int32)[None, :]).astype(jnp.int32)
    before = jnp.cumsum(chosen, axis=0) - chosen
    rank_in = jnp.sum(before * chosen, axis=1)
    return (flat_ids * SLOTS + rank_in).reshape(route_ids.shape)


def local(
    residual,
    queries,
    key_rows,
    value_rows,
    gate_rows,
    log_decay,
    out_gain,
    out_weight,
    norm_gain,
    expert_gate,
    expert_up,
    expert_down,
    routes,
    route_weight,
):
    length, head_dim = queries.shape
    sp_count = lax.axis_size(SP)
    tp = lax.axis_index("tp")
    tp_count = lax.axis_size("tp")
    positions = (lax.axis_index(SP) * length + jnp.arange(length, dtype=jnp.int32)).astype(F32)
    inverse = rope_base ** (-jnp.arange(0, head_dim, 2, dtype=F32) / head_dim)
    angles = positions[:, None] * inverse[None, :]
    cosine, sine = jnp.cos(angles), jnp.sin(angles)
    rotated_keys = rotate(key_rows.astype(F32), cosine, sine).astype(BF)
    cumulative = jnp.cumsum(log_decay, axis=1)[0]
    total = cumulative[-1]
    damped_keys = (rotated_keys.astype(F32) * jnp.exp(total - cumulative)[:, None]).astype(BF)
    block_state = lax.dot_general(
        damped_keys, value_rows, (((0,), (0,)), ((), ())), preferred_element_type=F32
    )
    carried = carried_in(total, block_state)

    rotated_queries = (rotate(queries.astype(F32), cosine, sine) * head_dim**-0.5).astype(BF)
    score_matrix = lax.dot_general(
        rotated_queries, rotated_keys, (((1,), (1,)), ((), ())), preferred_element_type=F32
    )
    causal = jnp.arange(length)[:, None] >= jnp.arange(length)[None, :]
    spread = cumulative[:, None] - cumulative[None, :]
    decays = jnp.where(causal, jnp.exp(jnp.where(causal, spread, 0.0)), 0.0)
    within = dot((score_matrix * decays).astype(BF), value_rows)
    readout = dot(rotated_queries.astype(F32), carried)
    head_out = within + jnp.exp(cumulative)[:, None] * readout
    head_norm = head_out * lax.rsqrt(
        jnp.mean(head_out * head_out, axis=-1, keepdims=True) + epsilon
    )
    mixed = (head_norm * out_gain[None, :] * jax.nn.silu(gate_rows.astype(F32))).astype(BF)

    held = out_weight
    same_core = jnp.concatenate(
        [held, shift(held, DOWN), shift(held, ACROSS), shift(held, UP)], axis=0
    )
    other_core = shift(same_core, OTHER_CORE)

    row_count, model_width = residual.shape
    heads = lax.all_to_all(
        mixed.reshape(tp_count, row_count, head_dim), "tp", split_axis=0, concat_axis=0, tiled=True
    )
    chip, core = tp // 2, tp % 2
    turned = lax.dynamic_slice_in_dim(jnp.concatenate([heads, heads]), 2 * chip, tp_count, 0)
    turned = turned.reshape(tp_count // 2, 2, row_count, head_dim)
    mine = jnp.where(core == 0, turned[:, 0], turned[:, 1])
    others = jnp.where(core == 0, turned[:, 1], turned[:, 0])

    def side_by_side(a):
        return jnp.concatenate([a[k] for k in range(a.shape[0])], axis=-1)

    projected = dot(side_by_side(mine), same_core) + dot(side_by_side(others), other_core)
    hidden_res = (residual.astype(F32) + projected).astype(BF)
    hidden_f = hidden_res.astype(F32)
    normed = (
        hidden_f
        * lax.rsqrt(jnp.mean(hidden_f * hidden_f, axis=-1, keepdims=True) + epsilon)
        * norm_gain[None, :]
    ).astype(BF)

    slots = slot_indices(routes, sp_count)
    packed_shape = (sp_count * SLOTS, USED * TAIL)
    message = (sp_count, SLOTS, USED * TAIL)
    packed = vmem_call(pack_tokens_kernel, jax.ShapeDtypeStruct(packed_shape, BF))(normed, slots.T)
    landed = lax.all_to_all(packed.reshape(message), SP, 0, 0, tiled=True)
    half = jax.ShapeDtypeStruct((sp_count * USED // 2, model_width), BF)
    low, high = vmem_call(unpack_rows_kernel, [half, half])(landed.reshape(packed_shape))
    low_parts, high_parts = routed_experts(low, high, expert_gate, expert_up, expert_down)
    repacked = vmem_call(repack_rows_kernel, jax.ShapeDtypeStruct(packed_shape, BF))(
        *low_parts, *high_parts
    )
    returned = lax.all_to_all(repacked.reshape(message), SP, 0, 0, tiled=True)
    return vmem_call(combine_kernel, jax.ShapeDtypeStruct(residual.shape, BF))(
        returned.reshape(packed_shape), hidden_res, slots, route_weight
    )


def solution(mesh):
    split = Mesh(mesh.devices.reshape(8, 4, mesh.shape["tp"]), ("sp_0", "sp_1", "tp"))
    in_specs = (
        P(SP_TP, None),
        P(SP, "tp"),
        P(SP, "tp"),
        P(SP, "tp"),
        P(SP, "tp"),
        P("tp", SP),
        P("tp"),
        P("tp", None),
        P(),
        P(SP, None, "tp"),
        P(SP, None, "tp"),
        P(SP, "tp", None),
        P(SP_TP, None),
        P(SP_TP, None),
    )
    out_specs = P(SP_TP, None)
    return jax.shard_map(local, mesh=split, in_specs=in_specs, out_specs=out_specs, check_vma=False)
```

```python
import jax
import jax.numpy as jnp
from jax import lax
from jax.experimental import pallas as pl
from jax.experimental.pallas import tpu as pltpu
from jax.sharding import Mesh
from jax.sharding import PartitionSpec as P


SP = ("sp_0", "sp_1")
SP_TP = ("sp_0", "sp_1", "tp")


epsilon = 1e-06
rope_base = 10000.0
BF = jnp.bfloat16
F32 = jnp.float32

OTHER_CORE = [(i, i ^ 1) for i in range(8)]
UP = [(i, (i + 2) % 8) for i in range(8)]
DOWN = [(i, (i - 2) % 8) for i in range(8)]
ACROSS = [(i, (i + 4) % 8) for i in range(8)]

SLOTS = 8
USED = 7
TAIL = 256


def dot(a, b):
    return jnp.dot(a, b, preferred_element_type=F32)


def vmem_call(kernel, out_shape, limit=12 * 1024 * 1024, **kwargs):
    return pl.pallas_call(
        kernel,
        out_shape=out_shape,
        compiler_params=pltpu.CompilerParams(vmem_limit_bytes=limit),
        **kwargs,
    )


def onehot(mask):
    return jnp.where(mask, 1.0, 0.0).astype(BF)


def project_and_pack_kernel(*refs):
    mine_ref, others_ref = refs[:2]
    weights = refs[2:10]
    residual_ref, gain_ref, slot_ref, hidden_ref, out_ref = refs[10:]
    tokens, width = residual_ref.shape
    heads = jnp.concatenate([ref[k] for ref in (mine_ref, others_ref) for k in range(4)], axis=1)
    squares = jnp.zeros((tokens, 1), F32)
    step = 512
    for start in range(0, width, step):
        columns = slice(start, start + step)
        projected = dot(heads, jnp.concatenate([w[:, columns] for w in weights], axis=0))
        hidden = (residual_ref[:, columns].astype(F32) + projected).astype(BF)
        hidden_ref[:, columns] = hidden
        hidden_f = hidden.astype(F32)
        squares = squares + jnp.sum(hidden_f * hidden_f, axis=1, keepdims=True)
    scale = lax.rsqrt(squares / width + epsilon)

    def normed(columns):
        return (hidden_ref[:, columns].astype(F32) * scale * gain_ref[:, columns]).astype(BF)

    rows = lax.broadcasted_iota(jnp.int32, (out_ref.shape[0], tokens), 0)
    first, second = slot_ref[0:1, :], slot_ref[1:2, :]
    place = rows & 7
    main_row = jnp.where(place < USED, rows, -1)
    main = onehot((main_row == first) | (main_row == second))
    tail_x = normed(slice(USED * TAIL, width))
    for r in range(USED):
        tail_row = jnp.where(place == USED, rows - USED + r, -1)
        tail = onehot((tail_row == first) | (tail_row == second))
        columns = slice(r * TAIL, (r + 1) * TAIL)
        out_ref[:, columns] = (dot(main, normed(columns)) + dot(tail, tail_x)).astype(BF)


def unpack_rows_kernel(in_ref, low_ref, high_ref):
    half = low_ref.shape[0]
    senders = in_ref.shape[0] // SLOTS
    for k, ref in enumerate((low_ref, high_ref)):
        p = lax.broadcasted_iota(jnp.int32, (half, in_ref.shape[0]), 0) + k * half
        q = lax.broadcasted_iota(jnp.int32, (half, in_ref.shape[0]), 1)
        chosen = onehot(q == (p & (senders - 1)) * SLOTS + p // senders)
        for r in range(USED):
            columns = slice(r * TAIL, (r + 1) * TAIL)
            ref[:, columns] = dot(chosen, in_ref[:, columns]).astype(BF)
        total = jnp.zeros((half, TAIL), F32)
        for r in range(USED):
            if (r + 1) * senders <= k * half or r * senders >= (k + 1) * half:
                continue
            tails = onehot((q == (p & (senders - 1)) * SLOTS + USED) & (p // senders == r))
            total = total + dot(tails, in_ref[:, r * TAIL : (r + 1) * TAIL])
        ref[:, USED * TAIL :] = total.astype(BF)


def repack_rows_kernel(*refs):
    out_ref = refs[-1]
    parts = refs[:-1]
    half = parts[0].shape[0]
    senders = out_ref.shape[0] // SLOTS
    count = len(parts) // 2
    q = lax.broadcasted_iota(jnp.int32, (out_ref.shape[0], half), 0)
    p = lax.broadcasted_iota(jnp.int32, (out_ref.shape[0], half), 1)
    place, sender = q & 7, q // SLOTS

    def summed(k, columns):
        total = parts[k * count][:, columns].astype(F32)
        for ref in parts[k * count + 1 : (k + 1) * count]:
            total = total + ref[:, columns].astype(F32)
        return total.astype(BF)

    main = [onehot((p + k * half == place * senders + sender) & (place < USED)) for k in (0, 1)]
    tail_rows = [summed(k, slice(USED * TAIL, None)) for k in (0, 1)]
    for r in range(USED):
        columns = slice(r * TAIL, (r + 1) * TAIL)
        total = jnp.zeros((out_ref.shape[0], TAIL), F32)
        for k in (0, 1):
            total = total + dot(main[k], summed(k, columns))
            if (r + 1) * senders <= k * half or r * senders >= (k + 1) * half:
                continue
            tail = onehot((p + k * half == r * senders + sender) & (place == USED))
            total = total + dot(tail, tail_rows[k])
        out_ref[:, columns] = total.astype(BF)


def combine_kernel(rows_ref, hidden_ref, slot_ref, weight_ref, out_ref):
    tokens = hidden_ref.shape[0]
    q = lax.broadcasted_iota(jnp.int32, (tokens, rows_ref.shape[0]), 1)

    def split(w):
        high = w.astype(BF)
        return high, (w - high.astype(F32)).astype(BF)

    pairs = [(slot_ref[:, k : k + 1], weight_ref[:, k : k + 1]) for k in (0, 1)]
    high, low = split(sum(jnp.where(q == s, w, 0.0) for s, w in pairs))
    tail = jnp.zeros((tokens, TAIL), F32)
    for r in range(USED):
        columns = slice(r * TAIL, (r + 1) * TAIL)
        rows = rows_ref[:, columns]
        got = dot(high, rows) + dot(low, rows)
        out_ref[:, columns] = (hidden_ref[:, columns].astype(F32) + got).astype(BF)
        tail_high, tail_low = split(
            sum(jnp.where((q == s - r + USED) & ((s & 7) == r), w, 0.0) for s, w in pairs)
        )
        tail = tail + dot(tail_high, rows) + dot(tail_low, rows)
    columns = slice(USED * TAIL, None)
    out_ref[:, columns] = (hidden_ref[:, columns].astype(F32) + tail).astype(BF)


def expert_kernel(*refs, count):
    parts = refs[:count]
    gate_ref, up_ref, down_ref = refs[count : count + 3]
    outs = refs[count + 3 : 2 * count + 3]
    rows, total = refs[2 * count + 3 :]
    step = pl.program_id(0)
    height = parts[0].shape[0]

    @pl.when(step == 0)
    def _():
        for k, part in enumerate(parts):
            rows[k * height : (k + 1) * height, :] = part[...]

    tile = rows.shape[0] // 2
    last = step == pl.num_programs(0) - 1

    def one_tile(k, carry):
        place = pl.ds(k * tile, tile)
        x = rows[place, :]
        hidden = (jax.nn.silu(dot(x, gate_ref[0])) * dot(x, up_ref[0])).astype(BF)
        piece = dot(hidden, down_ref[0])

        @pl.when(step == 0)
        def _():
            total[place, :] = piece

        @pl.when(last)
        def _():
            rows[place, :] = (total[place, :] + piece).astype(BF)

        return carry

    lax.fori_loop(0, 2, one_tile, 0)

    @pl.when(last)
    def _():
        for k, out in enumerate(outs):
            out[...] = rows[k * height : (k + 1) * height, :]


def expert(parts, gate, up, down):
    count = len(parts)
    height, width = parts[0].shape
    chunk = gate.shape[2] // 2
    part_spec = pl.BlockSpec((height, width), lambda j: (0, 0))
    return pl.pallas_call(
        lambda *refs: expert_kernel(*refs, count=count),
        grid=(2,),
        in_specs=[part_spec] * count
        + [
            pl.BlockSpec((1, width, chunk), lambda j: (0, 0, j)),
            pl.BlockSpec((1, width, chunk), lambda j: (0, 0, j)),
            pl.BlockSpec((1, chunk, width), lambda j: (0, j, 0)),
        ],
        out_specs=[part_spec] * count,
        out_shape=[jax.ShapeDtypeStruct((height, width), BF)] * count,
        scratch_shapes=[
            pltpu.VMEM((count * height, width), BF),
            pltpu.VMEM((count * height, width), F32),
        ],
        compiler_params=pltpu.CompilerParams(
            dimension_semantics=("arbitrary",), vmem_limit_bytes=24 * 1024 * 1024
        ),
        cost_estimate=pl.CostEstimate(
            flops=6 * count * height * width * gate.shape[2],
            bytes_accessed=2 * (2 * count * height * width + 3 * width * gate.shape[2]),
            transcendentals=count * height * gate.shape[2],
        ),
    )(*parts, gate, up, down)


def shift(a, where):
    return lax.ppermute(a, "tp", where)


def add(*parts):
    return sum(part.astype(F32) for part in parts).astype(BF)


def routed_experts(low, high, gate, up, down):
    def run(parts):
        return expert(parts, gate, up, down)

    below_low, above_high = shift(low, UP), shift(high, DOWN)
    other = [shift(a, OTHER_CORE) for a in (low, high)]
    below_high, above_low = shift(high, UP), shift(low, DOWN)
    own = run((low, high, *other))
    far_low, far_high = shift(below_low, UP), shift(above_high, DOWN)

    def both_cores(a, b):
        fetched = [shift(c, OTHER_CORE) for c in (a, b)]
        outs = run((a, b, *fetched))
        return [(outs[k], shift(outs[k + 2], OTHER_CORE)) for k in (0, 1)]

    first = both_cores(below_low, above_high)
    second = both_cores(below_high, above_low)
    far = both_cores(far_low, far_high)
    from_above_low = shift(add(*first[0]), DOWN)
    from_below_high = shift(add(*first[1]), UP)
    to_above_low = shift(add(*far[0]), UP)
    to_below_high = shift(add(*far[1]), DOWN)
    from_above_high = shift(add(*second[0], to_below_high), DOWN)
    from_below_low = shift(add(*second[1], to_above_low), UP)
    own_back = [shift(a, OTHER_CORE) for a in own[2:]]
    return (
        (own[0], own_back[0], from_below_low, from_above_low),
        (own[1], own_back[1], from_below_high, from_above_high),
    )


STATE = 136


def write_state(out_ref, total, state):
    high = total.astype(BF).astype(F32)
    row = lax.broadcasted_iota(jnp.int32, (8, state.shape[1]), 0)
    line = jnp.where(row == 0, high, jnp.where(row == 1, total - high, 0.0))
    message = jnp.concatenate([state, line], axis=0).astype(BF)
    for k in range(out_ref.shape[0]):
        out_ref[k] = message


def read_states(ref):
    size = ref.shape[2]
    states = [ref[k, :size, :].astype(F32) for k in range(ref.shape[0])]
    lines = [ref[k, size:, :].astype(F32) for k in range(ref.shape[0])]
    return [line[0:1, :] + line[1:2, :] for line in lines], states


def weighted(totals, states, end):
    result = jnp.zeros_like(states[0])
    between = jnp.zeros_like(totals[0])
    for k in reversed(range(len(states))):
        result = result + jnp.where(k < end, jnp.exp(between), 0.0) * states[k]
        between = between + jnp.where(k < end, totals[k], 0.0)
    return result, between


def block_state_kernel(
    key_ref, value_ref, decay_ref, cos_ref, sin_ref, rotated_ref, row_ref, column_ref, out_ref
):
    decay = decay_ref[...]
    blocks, width = decay.shape
    high = decay.astype(BF).astype(F32)
    middle = (decay - high).astype(BF).astype(F32)
    words = jnp.concatenate([high, middle, decay - high - middle], axis=0).astype(BF)
    upper = onehot(
        lax.broadcasted_iota(jnp.int32, (width, width), 0)
        <= lax.broadcasted_iota(jnp.int32, (width, width), 1)
    )
    sums = dot(words, upper)
    sums = sums[:blocks] + sums[blocks : 2 * blocks] + sums[2 * blocks :]
    total = jnp.zeros((1, 1), F32)
    rows = []
    for k in range(row_ref.shape[1] // width):
        rows.append(sums[k : k + 1, :] + total)
        total = rows[-1][:, width - 1 :]
    row_ref[...] = jnp.concatenate(rows, axis=1)
    column = jnp.concatenate([jnp.broadcast_to(r, (width, width)).T for r in rows], axis=0)
    column_ref[...] = column
    keys = key_ref[...].astype(F32)
    rotated = (keys * cos_ref[...] + pltpu.roll(keys, width // 2, 1) * sin_ref[...]).astype(BF)
    rotated_ref[...] = rotated
    damped = (rotated.astype(F32) * jnp.exp(total - column)).astype(BF)
    state = lax.dot_general(
        damped, value_ref[...], (((0,), (0,)), ((), ())), preferred_element_type=F32
    )
    write_state(out_ref, total, state)


def chip_row_kernel(in_ref, index_ref, inside_ref, ahead_ref, out_ref):
    totals, states = read_states(in_ref)
    inside, ahead = weighted(totals, states, index_ref[...])
    inside_ref[...] = inside
    ahead_ref[...] = ahead
    state, total = weighted(totals, states, len(states))
    write_state(out_ref, total, state)


def within_kernel(query_ref, rotated_ref, value_ref, row_ref, column_ref, cos_ref, sin_ref, turned_ref, out_ref):
    width = query_ref.shape[1]
    queries = query_ref[...].astype(F32)
    turned = queries * cos_ref[...] + pltpu.roll(queries, width // 2, 1) * sin_ref[...]
    turned_ref[...] = (turned * width**-0.5).astype(BF)
    step = 256
    for start in range(0, query_ref.shape[0], step):
        end = start + step
        scores = lax.dot_general(
            turned_ref[start:end, :],
            rotated_ref[:end, :],
            (((1,), (1,)), ((), ())),
            preferred_element_type=F32,
        )
        i = lax.broadcasted_iota(jnp.int32, scores.shape, 0) + start
        causal = i >= lax.broadcasted_iota(jnp.int32, scores.shape, 1)
        spread = column_ref[start:end, 0:1] - row_ref[:, :end]
        decays = jnp.where(causal, jnp.exp(jnp.where(causal, spread, 0.0)), 0.0)
        out_ref[start:end, :] = dot((scores * decays).astype(BF), value_ref[:end, :])


def mix_kernel(
    in_ref, index_ref, inside_ref, ahead_ref, turned_ref, within_ref, column_ref, gate_ref, gain_ref, out_ref
):
    totals, states = read_states(in_ref)
    before, _ = weighted(totals, states, index_ref[...])
    carried = jnp.exp(ahead_ref[...]) * before + inside_ref[...]
    high = carried.astype(BF)
    low = (carried - high.astype(F32)).astype(BF)
    turned = turned_ref[...]
    readout = dot(turned, high) + dot(turned, low)
    out = within_ref[...] + jnp.exp(column_ref[...]) * readout
    scale = lax.rsqrt(jnp.mean(out * out, axis=1, keepdims=True) + epsilon)
    gate = gate_ref[...].astype(F32)
    out_ref[...] = (out * scale * gain_ref[...] * jax.nn.silu(gate)).astype(BF)


def slot_indices(route_ids, experts):
    flat_ids = route_ids.reshape(-1)
    chosen = (flat_ids[:, None] == jnp.arange(experts, dtype=jnp.int32)[None, :]).astype(jnp.int32)
    before = jnp.cumsum(chosen, axis=0) - chosen
    rank_in = jnp.sum(before * chosen, axis=1)
    return (flat_ids * SLOTS + rank_in).reshape(route_ids.shape)


def layer(
    residual,
    queries,
    key_rows,
    value_rows,
    gate_rows,
    log_decay,
    out_gain,
    out_weight,
    norm_gain,
    expert_gate,
    expert_up,
    expert_down,
    routes,
    route_weight,
):
    length, head_dim = queries.shape
    sp_count = lax.axis_size(SP)
    tp = lax.axis_index("tp")
    tp_count = lax.axis_size("tp")
    positions = (lax.axis_index(SP) * length + jnp.arange(length, dtype=jnp.int32)).astype(F32)
    column = jnp.arange(head_dim)
    half_dim = head_dim // 2
    inverse = rope_base ** (-(2 * (column % half_dim)).astype(F32) / head_dim)
    angles = positions[:, None] * inverse[None, :]
    cosine = jnp.cos(angles)
    sine = jnp.sin(angles) * jnp.where(column < half_dim, -1.0, 1.0)[None, :]
    shape = jax.ShapeDtypeStruct
    decay_rows = jnp.pad(log_decay.reshape(-1, head_dim), ((0, 2), (0, 0)))
    rotated_keys, decay_row, decay_column, message = vmem_call(
        block_state_kernel,
        [
            shape((length, head_dim), BF),
            shape((1, length), F32),
            shape((length, head_dim), F32),
            shape((lax.axis_size("sp_1"), STATE, head_dim), BF),
        ],
    )(key_rows, value_rows, decay_rows, cosine, sine)
    pieces = lax.all_to_all(message, "sp_1", 0, 0, tiled=True)
    rotated_queries, within = vmem_call(
        within_kernel,
        [shape((length, head_dim), BF), shape((length, head_dim), F32)],
        cost_estimate=pl.CostEstimate(
            flops=3 * length * length * head_dim,
            bytes_accessed=12 * length * head_dim,
            transcendentals=length * length,
        ),
    )(queries, rotated_keys, value_rows, decay_row, decay_column, cosine, sine)

    def index_line(axis):
        return jnp.full((1, head_dim), lax.axis_index(axis), jnp.int32)

    inside, ahead, message = vmem_call(
        chip_row_kernel,
        [
            shape((head_dim, head_dim), F32),
            shape((1, head_dim), F32),
            shape((lax.axis_size("sp_0"), STATE, head_dim), BF),
        ],
    )(pieces, index_line("sp_1"))
    pieces = lax.all_to_all(message, "sp_0", 0, 0, tiled=True)
    mixed = vmem_call(mix_kernel, shape((length, head_dim), BF))(
        pieces,
        index_line("sp_0"),
        inside,
        ahead,
        rotated_queries,
        within,
        decay_column,
        gate_rows,
        out_gain[None],
    )

    weights = [
        out_weight, shift(out_weight, DOWN), shift(out_weight, ACROSS), shift(out_weight, UP)
    ]
    weights = weights + [shift(w, OTHER_CORE) for w in weights]

    row_count, model_width = residual.shape
    heads = lax.all_to_all(
        mixed.reshape(tp_count, row_count, head_dim), "tp", 0, 0, tiled=True
    )
    chip, core = tp // 2, tp % 2
    turned = lax.dynamic_slice_in_dim(jnp.concatenate([heads, heads]), 2 * chip, tp_count, 0)
    turned = turned.reshape(tp_count // 2, 2, row_count, head_dim)
    mine = jnp.where(core == 0, turned[:, 0], turned[:, 1])
    others = jnp.where(core == 0, turned[:, 1], turned[:, 0])

    slots = slot_indices(routes, sp_count)
    packed_shape = (sp_count * SLOTS, USED * TAIL)
    message = (sp_count, SLOTS, USED * TAIL)
    hidden_res, packed = vmem_call(
        project_and_pack_kernel,
        [shape((row_count, model_width), BF), shape(packed_shape, BF)],
    )(mine, others, *weights, residual, norm_gain[None], slots.T)
    landed = lax.all_to_all(packed.reshape(message), SP, 0, 0, tiled=True)
    half = jax.ShapeDtypeStruct((sp_count * USED // 2, model_width), BF)
    low, high = vmem_call(unpack_rows_kernel, [half, half])(landed.reshape(packed_shape))
    low_parts, high_parts = routed_experts(low, high, expert_gate, expert_up, expert_down)
    repacked = vmem_call(repack_rows_kernel, jax.ShapeDtypeStruct(packed_shape, BF))(
        *low_parts, *high_parts
    )
    returned = lax.all_to_all(repacked.reshape(message), SP, 0, 0, tiled=True)
    return vmem_call(combine_kernel, jax.ShapeDtypeStruct(residual.shape, BF))(
        returned.reshape(packed_shape), hidden_res, slots, route_weight
    )


def solution(mesh):
    split = Mesh(mesh.devices.reshape(8, 4, mesh.shape["tp"]), ("sp_0", "sp_1", "tp"))
    in_specs = (
        P(SP_TP, None),
        P(SP, "tp"),
        P(SP, "tp"),
        P(SP, "tp"),
        P(SP, "tp"),
        P("tp", SP),
        P("tp"),
        P("tp", None),
        P(),
        P(SP, None, "tp"),
        P(SP, None, "tp"),
        P(SP, "tp", None),
        P(SP_TP, None),
        P(SP_TP, None),
    )
    out_specs = P(SP_TP, None)
    return jax.shard_map(layer, mesh=split, in_specs=in_specs, out_specs=out_specs, check_vma=False)
```

```python
import jax
import jax.numpy as jnp
from jax import lax
from jax.experimental import pallas as pl
from jax.experimental.pallas import tpu as pltpu
from jax.sharding import Mesh
from jax.sharding import PartitionSpec as P


SP = ("sp_0", "sp_1")
SP_TP = ("sp_0", "sp_1", "tp")


epsilon = 1e-06
rope_base = 10000.0
BF = jnp.bfloat16
F32 = jnp.float32

OTHER_CORE = [(i, i ^ 1) for i in range(8)]
UP = [(i, (i + 2) % 8) for i in range(8)]
DOWN = [(i, (i - 2) % 8) for i in range(8)]
ACROSS = [(i, (i + 4) % 8) for i in range(8)]

SLOTS = 8
USED = 7
UNIT = 16
BLOCK = 256


def dot(a, b):
    return jnp.dot(a, b, preferred_element_type=F32)


def vmem_call(kernel, out_shape, limit=12 * 1024 * 1024, **kwargs):
    return pl.pallas_call(
        kernel,
        out_shape=out_shape,
        compiler_params=pltpu.CompilerParams(vmem_limit_bytes=limit),
        **kwargs,
    )


def onehot(mask):
    return jnp.where(mask, 1.0, 0.0).astype(BF)


def by_block(size):
    peers = size // SLOTS
    to = lax.broadcasted_iota(jnp.int32, (size, size), 0)
    source = lax.broadcasted_iota(jnp.int32, (size, size), 1)
    return onehot(source == (to & (peers - 1)) * SLOTS + to // peers)


def by_peer(size):
    peers = size // SLOTS
    to = lax.broadcasted_iota(jnp.int32, (size, size), 0)
    source = lax.broadcasted_iota(jnp.int32, (size, size), 1)
    return onehot(source == (to & 7) * peers + to // SLOTS)


def slot_of_row(shape, dim, peers):
    row = lax.broadcasted_iota(jnp.int32, shape, dim)
    return (row & (peers - 1)) * SLOTS + row // peers


def project_and_pack_kernel(*refs):
    mine_ref, others_ref = refs[:2]
    weights = refs[2:10]
    residual_ref, gain_ref, slot_ref, hidden_ref, out_ref, turned = refs[10:]
    tokens, width = residual_ref.shape
    size = out_ref.shape[0]
    peers = size // SLOTS
    heads = jnp.concatenate([ref[k] for ref in (mine_ref, others_ref) for k in range(4)], axis=1)
    squares = jnp.zeros((tokens, 1), F32)
    step = 512
    for start in range(0, width, step):
        columns = slice(start, start + step)
        projected = dot(heads, jnp.concatenate([w[:, columns] for w in weights], axis=0))
        hidden = (residual_ref[:, columns].astype(F32) + projected).astype(BF)
        hidden_ref[:, columns] = hidden
        hidden_f = hidden.astype(F32)
        squares = squares + jnp.sum(hidden_f * hidden_f, axis=1, keepdims=True)
    scale = lax.rsqrt(squares / width + epsilon)
    slot = slot_of_row((USED * peers, tokens), 0, peers)
    chosen = onehot((slot == slot_ref[0:1, :]) | (slot == slot_ref[1:2, :]))
    for i in range(SLOTS):
        columns = slice(i * BLOCK, (i + 1) * BLOCK)
        normed = hidden_ref[:, columns].astype(F32) * scale * gain_ref[:, columns]
        picked = dot(chosen, normed.astype(BF)).astype(BF)
        for c in range(USED):
            turned[i * peers : (i + 1) * peers, c * BLOCK : (c + 1) * BLOCK] = picked[
                c * peers : (c + 1) * peers, :
            ]
    out_ref[...] = dot(by_peer(size), turned[...]).astype(BF)


def units(refs):
    for ref in refs:
        for start in range(0, ref.shape[0], UNIT):
            yield ref, slice(start, start + UNIT)


def unpack(in_ref, *out_refs):
    size = in_ref.shape[0]
    peers = size // SLOTS
    order = by_block(size)
    places = list(units(out_refs))
    each = peers // UNIT
    for c in range(in_ref.shape[1] // BLOCK):
        rows = dot(order, in_ref[:, c * BLOCK : (c + 1) * BLOCK]).astype(BF)
        for k in range(each):
            ref, place = places[c * each + k]
            for i in range(SLOTS):
                start = i * peers + k * UNIT
                ref[place, i * BLOCK : (i + 1) * BLOCK] = rows[start : start + UNIT, :]


def unpack_rows_kernel(in_ref, low_ref, high_ref, both_ref):
    unpack(in_ref, low_ref, high_ref)
    half = low_ref.shape[0]
    both_ref[:half, :] = low_ref[...]
    both_ref[half:, :] = high_ref[...]


def repack_rows_kernel(low_ref, high_ref, core_ref, *refs):
    *chips, out_ref, turned = refs
    size = out_ref.shape[0]
    peers = size // SLOTS
    each = peers // UNIT
    sources = [(low_ref, high_ref), (core_ref,), chips[0::2], chips[1::2]]
    for u, parts in enumerate(zip(*map(units, sources))):
        total = sum(ref[place, :].astype(F32) for ref, place in parts).astype(BF)
        c, start = u // each, u % each * UNIT
        for i in range(SLOTS):
            turned[i * peers + start : i * peers + start + UNIT, c * BLOCK : (c + 1) * BLOCK] = (
                total[:, i * BLOCK : (i + 1) * BLOCK]
            )
    out_ref[...] = dot(by_peer(size), turned[...]).astype(BF)


def add_kernel(own_ref, core_ref, *refs, start):
    *more, out_ref = refs
    total = own_ref[...].astype(F32) + core_ref[start : start + own_ref.shape[0], :].astype(F32)
    for ref in more:
        total = total + ref[...].astype(F32)
    out_ref[...] = total.astype(BF)


def add(own, core, second, *more):
    return vmem_call(
        lambda *refs: add_kernel(*refs, start=own.shape[0] * second),
        jax.ShapeDtypeStruct(own.shape, BF),
    )(own, core, *more)


def route_rows_kernel(slot_ref, weight_ref, high_ref, low_ref):
    slot = slot_of_row(high_ref.shape, 1, high_ref.shape[1] // USED)
    weight = sum(
        jnp.where(slot == slot_ref[:, k : k + 1], weight_ref[:, k : k + 1], 0.0) for k in (0, 1)
    )
    high = weight.astype(BF)
    high_ref[...] = high
    low_ref[...] = (weight - high.astype(F32)).astype(BF)


def combine_kernel(rows_ref, hidden_ref, high_ref, low_ref, out_ref, rows):
    unpack(rows_ref, rows)
    for i in range(SLOTS):
        columns = slice(i * BLOCK, (i + 1) * BLOCK)
        block = rows[:, columns]
        got = dot(high_ref[...], block) + dot(low_ref[...], block)
        out_ref[:, columns] = (hidden_ref[:, columns].astype(F32) + got).astype(BF)


def expert_kernel(*refs, count):
    parts = refs[:count]
    gate_ref, up_ref, down_ref = refs[count : count + 3]
    outs = refs[count + 3 : -2]
    rows, total = refs[-2:]
    step = pl.program_id(0)

    def places(pieces):
        start = 0
        for piece in pieces:
            yield slice(start, start + piece.shape[0])
            start += piece.shape[0]

    @pl.when(step == 0)
    def _():
        for part, place in zip(parts, places(parts)):
            rows[place, :] = part[...]

    tile = rows.shape[0] // 2
    last = step == pl.num_programs(0) - 1

    def one_tile(k, carry):
        place = pl.ds(k * tile, tile)
        x = rows[place, :]
        hidden = (jax.nn.silu(dot(x, gate_ref[0])) * dot(x, up_ref[0])).astype(BF)
        piece = dot(hidden, down_ref[0])

        @pl.when(step == 0)
        def _():
            total[place, :] = piece

        @pl.when(last)
        def _():
            rows[place, :] = (total[place, :] + piece).astype(BF)

        return carry

    lax.fori_loop(0, 2, one_tile, 0)

    @pl.when(last)
    def _():
        for out, place in zip(outs, places(outs)):
            out[...] = rows[place, :]


def expert(parts, gate, up, down):
    count = len(parts)
    height = sum(part.shape[0] for part in parts)
    width = parts[0].shape[1]
    chunk = gate.shape[2] // 2
    outs = [parts[0].shape, parts[1].shape, (height // 2, width)]

    def whole(shape):
        return pl.BlockSpec(shape, lambda j: (0, 0))

    return pl.pallas_call(
        lambda *refs: expert_kernel(*refs, count=count),
        grid=(2,),
        in_specs=[whole(part.shape) for part in parts]
        + [
            pl.BlockSpec((1, width, chunk), lambda j: (0, 0, j)),
            pl.BlockSpec((1, width, chunk), lambda j: (0, 0, j)),
            pl.BlockSpec((1, chunk, width), lambda j: (0, j, 0)),
        ],
        out_specs=[whole(out) for out in outs],
        out_shape=[jax.ShapeDtypeStruct(out, BF) for out in outs],
        scratch_shapes=[pltpu.VMEM((height, width), BF), pltpu.VMEM((height, width), F32)],
        compiler_params=pltpu.CompilerParams(
            dimension_semantics=("arbitrary",), vmem_limit_bytes=20 * 1024 * 1024
        ),
        cost_estimate=pl.CostEstimate(
            flops=6 * height * width * gate.shape[2],
            bytes_accessed=2 * (2 * height * width + 3 * width * gate.shape[2]),
            transcendentals=height * gate.shape[2],
        ),
    )(*parts, gate, up, down)


def shift(a, where):
    return lax.ppermute(a, "tp", where)


def routed_experts(low, high, both, gate, up, down):
    def run(*parts):
        return expert(parts, gate, up, down)

    below_low, above_high = shift(low, UP), shift(high, DOWN)
    other = shift(both, OTHER_CORE)
    below_high, above_low = shift(high, UP), shift(low, DOWN)
    own_low, own_high, own = run(low, high, other)
    far_low, far_high = shift(below_low, UP), shift(above_high, DOWN)

    def both_cores(a, b):
        fetched = [shift(c, OTHER_CORE) for c in (a, b)]
        out_a, out_b, others = run(a, b, *fetched)
        back = shift(others, OTHER_CORE)
        return (out_a, back, 0), (out_b, back, 1)

    first = both_cores(below_low, above_high)
    second = both_cores(below_high, above_low)
    far = both_cores(far_low, far_high)
    from_above_low = shift(add(*first[0]), DOWN)
    from_below_high = shift(add(*first[1]), UP)
    to_above_low = shift(add(*far[0]), UP)
    to_below_high = shift(add(*far[1]), DOWN)
    from_above_high = shift(add(*second[0], to_below_high), DOWN)
    from_below_low = shift(add(*second[1], to_above_low), UP)
    own_back = shift(own, OTHER_CORE)
    return (
        own_low,
        own_high,
        own_back,
        from_below_low,
        from_above_low,
        from_below_high,
        from_above_high,
    )


STATE = 136


def write_state(out_ref, total, state):
    high = total.astype(BF).astype(F32)
    row = lax.broadcasted_iota(jnp.int32, (8, state.shape[1]), 0)
    line = jnp.where(row == 0, high, jnp.where(row == 1, total - high, 0.0))
    message = jnp.concatenate([state, line], axis=0).astype(BF)
    for k in range(out_ref.shape[0]):
        out_ref[k] = message


def read_states(ref):
    size = ref.shape[2]
    states = [ref[k, :size, :].astype(F32) for k in range(ref.shape[0])]
    lines = [ref[k, size:, :].astype(F32) for k in range(ref.shape[0])]
    return [line[0:1, :] + line[1:2, :] for line in lines], states


def weighted(totals, states, end):
    result = jnp.zeros_like(states[0])
    between = jnp.zeros_like(totals[0])
    for k in reversed(range(len(states))):
        result = result + jnp.where(k < end, jnp.exp(between), 0.0) * states[k]
        between = between + jnp.where(k < end, totals[k], 0.0)
    return result, between


def block_state_kernel(
    key_ref, value_ref, decay_ref, cos_ref, sin_ref, rotated_ref, row_ref, column_ref, out_ref
):
    decay = decay_ref[...]
    blocks, width = decay.shape
    high = decay.astype(BF).astype(F32)
    middle = (decay - high).astype(BF).astype(F32)
    words = jnp.concatenate([high, middle, decay - high - middle], axis=0).astype(BF)
    upper = onehot(
        lax.broadcasted_iota(jnp.int32, (width, width), 0)
        <= lax.broadcasted_iota(jnp.int32, (width, width), 1)
    )
    sums = dot(words, upper)
    sums = sums[:blocks] + sums[blocks : 2 * blocks] + sums[2 * blocks :]
    total = jnp.zeros((1, 1), F32)
    rows = []
    for k in range(row_ref.shape[1] // width):
        rows.append(sums[k : k + 1, :] + total)
        total = rows[-1][:, width - 1 :]
    row_ref[...] = jnp.concatenate(rows, axis=1)
    column = jnp.concatenate([jnp.broadcast_to(r, (width, width)).T for r in rows], axis=0)
    column_ref[...] = column
    keys = key_ref[...].astype(F32)
    rotated = (keys * cos_ref[...] + pltpu.roll(keys, width // 2, 1) * sin_ref[...]).astype(BF)
    rotated_ref[...] = rotated
    damped = (rotated.astype(F32) * jnp.exp(total - column)).astype(BF)
    state = lax.dot_general(
        damped, value_ref[...], (((0,), (0,)), ((), ())), preferred_element_type=F32
    )
    write_state(out_ref, total, state)


def chip_row_kernel(in_ref, index_ref, inside_ref, ahead_ref, out_ref):
    totals, states = read_states(in_ref)
    inside, ahead = weighted(totals, states, index_ref[...])
    inside_ref[...] = inside
    ahead_ref[...] = ahead
    state, total = weighted(totals, states, len(states))
    write_state(out_ref, total, state)


def within_kernel(query_ref, rotated_ref, value_ref, row_ref, column_ref, cos_ref, sin_ref, turned_ref, out_ref):
    width = query_ref.shape[1]
    queries = query_ref[...].astype(F32)
    turned = queries * cos_ref[...] + pltpu.roll(queries, width // 2, 1) * sin_ref[...]
    turned_ref[...] = (turned * width**-0.5).astype(BF)
    step = 256

    def some_rows(k, carry):
        place = pl.ds(k * step, step)
        scores = lax.dot_general(
            turned_ref[place, :],
            rotated_ref[...],
            (((1,), (1,)), ((), ())),
            preferred_element_type=F32,
        )
        i = lax.broadcasted_iota(jnp.int32, scores.shape, 0) + k * step
        causal = i >= lax.broadcasted_iota(jnp.int32, scores.shape, 1)
        spread = column_ref[place, 0:1] - row_ref[...]
        decays = jnp.where(causal, jnp.exp(jnp.where(causal, spread, 0.0)), 0.0)
        out_ref[place, :] = dot((scores * decays).astype(BF), value_ref[...])
        return carry

    lax.fori_loop(0, query_ref.shape[0] // step, some_rows, 0)


def mix_kernel(
    in_ref, index_ref, inside_ref, ahead_ref, turned_ref, within_ref, column_ref, gate_ref, gain_ref, out_ref
):
    totals, states = read_states(in_ref)
    before, _ = weighted(totals, states, index_ref[...])
    carried = jnp.exp(ahead_ref[...]) * before + inside_ref[...]
    high = carried.astype(BF)
    low = (carried - high.astype(F32)).astype(BF)
    turned = turned_ref[...]
    readout = dot(turned, high) + dot(turned, low)
    out = within_ref[...] + jnp.exp(column_ref[...]) * readout
    scale = lax.rsqrt(jnp.mean(out * out, axis=1, keepdims=True) + epsilon)
    gate = gate_ref[...].astype(F32)
    out_ref[...] = (out * scale * gain_ref[...] * jax.nn.silu(gate)).astype(BF)


def slot_indices(route_ids, experts):
    flat_ids = route_ids.reshape(-1)
    chosen = (flat_ids[:, None] == jnp.arange(experts, dtype=jnp.int32)[None, :]).astype(jnp.int32)
    before = jnp.cumsum(chosen, axis=0) - chosen
    rank_in = jnp.sum(before * chosen, axis=1)
    return (flat_ids * SLOTS + rank_in).reshape(route_ids.shape)


def layer(
    residual,
    queries,
    key_rows,
    value_rows,
    gate_rows,
    log_decay,
    out_gain,
    out_weight,
    norm_gain,
    expert_gate,
    expert_up,
    expert_down,
    routes,
    route_weight,
):
    length, head_dim = queries.shape
    sp_count = lax.axis_size(SP)
    tp = lax.axis_index("tp")
    tp_count = lax.axis_size("tp")
    positions = (lax.axis_index(SP) * length + jnp.arange(length, dtype=jnp.int32)).astype(F32)
    column = jnp.arange(head_dim)
    half_dim = head_dim // 2
    inverse = rope_base ** (-(2 * (column % half_dim)).astype(F32) / head_dim)
    angles = positions[:, None] * inverse[None, :]
    cosine = jnp.cos(angles)
    sine = jnp.sin(angles) * jnp.where(column < half_dim, -1.0, 1.0)[None, :]
    shape = jax.ShapeDtypeStruct
    decay_rows = jnp.pad(log_decay.reshape(-1, head_dim), ((0, 2), (0, 0)))
    rotated_keys, decay_row, decay_column, message = vmem_call(
        block_state_kernel,
        [
            shape((length, head_dim), BF),
            shape((1, length), F32),
            shape((length, head_dim), F32),
            shape((lax.axis_size("sp_1"), STATE, head_dim), BF),
        ],
    )(key_rows, value_rows, decay_rows, cosine, sine)
    pieces = lax.all_to_all(message, "sp_1", 0, 0, tiled=True)
    rotated_queries, within = vmem_call(
        within_kernel,
        [shape((length, head_dim), BF), shape((length, head_dim), F32)],
        cost_estimate=pl.CostEstimate(
            flops=3 * length * length * head_dim,
            bytes_accessed=12 * length * head_dim,
            transcendentals=length * length,
        ),
    )(queries, rotated_keys, value_rows, decay_row, decay_column, cosine, sine)

    def index_line(axis):
        return jnp.full((1, head_dim), lax.axis_index(axis), jnp.int32)

    inside, ahead, message = vmem_call(
        chip_row_kernel,
        [
            shape((head_dim, head_dim), F32),
            shape((1, head_dim), F32),
            shape((lax.axis_size("sp_0"), STATE, head_dim), BF),
        ],
    )(pieces, index_line("sp_1"))
    pieces = lax.all_to_all(message, "sp_0", 0, 0, tiled=True)
    mixed = vmem_call(mix_kernel, shape((length, head_dim), BF))(
        pieces,
        index_line("sp_0"),
        inside,
        ahead,
        rotated_queries,
        within,
        decay_column,
        gate_rows,
        out_gain[None],
    )

    weights = [
        out_weight, shift(out_weight, DOWN), shift(out_weight, ACROSS), shift(out_weight, UP)
    ]
    weights = weights + [shift(w, OTHER_CORE) for w in weights]

    row_count, model_width = residual.shape
    heads = lax.all_to_all(
        mixed.reshape(tp_count, row_count, head_dim), "tp", 0, 0, tiled=True
    )
    chip, core = tp // 2, tp % 2
    turned = lax.dynamic_slice_in_dim(jnp.concatenate([heads, heads]), 2 * chip, tp_count, 0)
    turned = turned.reshape(tp_count // 2, 2, row_count, head_dim)
    mine = jnp.where(core == 0, turned[:, 0], turned[:, 1])
    others = jnp.where(core == 0, turned[:, 1], turned[:, 0])

    slots = slot_indices(routes, sp_count)
    size = sp_count * SLOTS
    packed = shape((size, USED * BLOCK), BF)
    message = (sp_count, SLOTS, USED * BLOCK)
    turning = [pltpu.VMEM(packed.shape, BF)]
    hidden_res, tokens = vmem_call(
        project_and_pack_kernel,
        [shape((row_count, model_width), BF), packed],
        scratch_shapes=turning,
    )(mine, others, *weights, residual, norm_gain[None], slots.T)
    landed = lax.all_to_all(tokens.reshape(message), SP, 0, 0, tiled=True)
    half = shape((sp_count * USED // 2, model_width), BF)
    rows = vmem_call(
        unpack_rows_kernel, [half, half, shape((sp_count * USED, model_width), BF)]
    )(landed.reshape(packed.shape))
    route = shape((row_count, sp_count * USED), BF)
    high_weight, low_weight = vmem_call(route_rows_kernel, [route, route])(slots, route_weight)
    parts = routed_experts(*rows, expert_gate, expert_up, expert_down)
    repacked = vmem_call(repack_rows_kernel, packed, scratch_shapes=turning)(*parts)
    returned = lax.all_to_all(repacked.reshape(message), SP, 0, 0, tiled=True)
    return vmem_call(
        combine_kernel,
        shape(residual.shape, BF),
        scratch_shapes=[pltpu.VMEM((sp_count * USED, model_width), BF)],
    )(returned.reshape(packed.shape), hidden_res, high_weight, low_weight)


def solution(mesh):
    split = Mesh(mesh.devices.reshape(8, 4, mesh.shape["tp"]), ("sp_0", "sp_1", "tp"))
    in_specs = (
        P(SP_TP, None),
        P(SP, "tp"),
        P(SP, "tp"),
        P(SP, "tp"),
        P(SP, "tp"),
        P("tp", SP),
        P("tp"),
        P("tp", None),
        P(),
        P(SP, None, "tp"),
        P(SP, None, "tp"),
        P(SP, "tp", None),
        P(SP_TP, None),
        P(SP_TP, None),
    )
    out_specs = P(SP_TP, None)
    return jax.shard_map(layer, mesh=split, in_specs=in_specs, out_specs=out_specs, check_vma=False)
```

```python
import jax
import jax.numpy as jnp
from jax import lax
from jax.experimental import pallas as pl
from jax.experimental.pallas import tpu as pltpu
from jax.sharding import Mesh
from jax.sharding import PartitionSpec as P


SP = ("sp_0", "sp_1")
SP_TP = ("sp_0", "sp_1", "tp")


epsilon = 1e-06
rope_base = 10000.0
BF = jnp.bfloat16
F32 = jnp.float32

OTHER_CORE = [(i, i ^ 1) for i in range(8)]
UP = [(i, (i + 2) % 8) for i in range(8)]
DOWN = [(i, (i - 2) % 8) for i in range(8)]
ACROSS = [(i, (i + 4) % 8) for i in range(8)]

SLOTS = 8
USED = 7
UNIT = 16
BLOCK = 256


def dot(a, b):
    return jnp.dot(a, b, preferred_element_type=F32)


def whole(shape):
    return pl.BlockSpec(shape, lambda j: (0,) * len(shape))


def vmem_call(kernel, out_shape, late=(), scratch_shapes=(), **kwargs):
    def call(*args):
        args = [
            pltpu.with_memory_space_constraint(a, pltpu.HBM) if k in late else a
            for k, a in enumerate(args)
        ]
        count = len(args)
        outs = len(jax.tree.leaves(out_shape))
        buffers = [pltpu.VMEM(args[k].shape, args[k].dtype) for k in late]
        signals = [pltpu.SemaphoreType.DMA(())] * len(late)

        def body(*refs):
            ins = list(refs[:count])
            rest = refs[count : count + outs + len(scratch_shapes)]
            extra = refs[count + outs + len(scratch_shapes) :]
            copies = []
            for n, k in enumerate(late):
                copies.append(pltpu.make_async_copy(ins[k], extra[n], extra[len(late) + n]))
                copies[-1].start()
                ins[k] = extra[n]

            def ready():
                for copy in copies:
                    copy.wait()

            if late:
                kernel(*ins, *rest, ready=ready)
            else:
                kernel(*ins, *rest)

        return pl.pallas_call(
            body,
            in_specs=[
                pl.BlockSpec(memory_space=pltpu.HBM if k in late else pltpu.VMEM)
                for k in range(count)
            ],
            out_shape=out_shape,
            scratch_shapes=[*scratch_shapes, *buffers, *signals],
            compiler_params=pltpu.CompilerParams(vmem_limit_bytes=12 * 1024 * 1024),
            **kwargs,
        )(*args)

    return call


def onehot(mask):
    return jnp.where(mask, 1.0, 0.0).astype(BF)


def by_block(size):
    peers = size // SLOTS
    to = lax.broadcasted_iota(jnp.int32, (size, size), 0)
    source = lax.broadcasted_iota(jnp.int32, (size, size), 1)
    return onehot(source == (to & (peers - 1)) * SLOTS + to // peers)


def by_peer(size):
    peers = size // SLOTS
    to = lax.broadcasted_iota(jnp.int32, (size, size), 0)
    source = lax.broadcasted_iota(jnp.int32, (size, size), 1)
    return onehot(source == (to & 7) * peers + to // SLOTS)


def slot_of_row(shape, dim, peers):
    row = lax.broadcasted_iota(jnp.int32, shape, dim)
    return (row & (peers - 1)) * SLOTS + row // peers


def project_and_pack_kernel(*refs, ready):
    mine_ref, others_ref = refs[:2]
    weights = refs[2:10]
    residual_ref, gain_ref, slot_ref, hidden_ref, out_ref, turned = refs[10:]
    tokens, width = residual_ref.shape
    size = out_ref.shape[0]
    peers = size // SLOTS
    heads = jnp.concatenate([ref[k] for ref in (mine_ref, others_ref) for k in range(4)], axis=1)
    squares = jnp.zeros((tokens, 1), F32)
    step = 512
    for start in range(0, width, step):
        columns = slice(start, start + step)
        projected = dot(heads, jnp.concatenate([w[:, columns] for w in weights], axis=0))
        if start == 0:
            ready()
        hidden = (residual_ref[:, columns].astype(F32) + projected).astype(BF)
        hidden_ref[:, columns] = hidden
        hidden_f = hidden.astype(F32)
        squares = squares + jnp.sum(hidden_f * hidden_f, axis=1, keepdims=True)
    scale = lax.rsqrt(squares / width + epsilon)
    slot = slot_of_row((USED * peers, tokens), 0, peers)
    chosen = onehot((slot == slot_ref[0:1, :]) | (slot == slot_ref[1:2, :]))
    for i in range(SLOTS):
        columns = slice(i * BLOCK, (i + 1) * BLOCK)
        normed = hidden_ref[:, columns].astype(F32) * scale * gain_ref[:, columns]
        picked = dot(chosen, normed.astype(BF)).astype(BF)
        for c in range(USED):
            turned[i * peers : (i + 1) * peers, c * BLOCK : (c + 1) * BLOCK] = picked[
                c * peers : (c + 1) * peers, :
            ]
    out_ref[...] = dot(by_peer(size), turned[...]).astype(BF)


def units(refs):
    for ref in refs:
        for start in range(0, ref.shape[0], UNIT):
            yield ref, slice(start, start + UNIT)


def unpack(in_ref, *out_refs):
    size = in_ref.shape[0]
    peers = size // SLOTS
    order = by_block(size)
    places = list(units(out_refs))
    each = peers // UNIT
    for c in range(in_ref.shape[1] // BLOCK):
        rows = dot(order, in_ref[:, c * BLOCK : (c + 1) * BLOCK]).astype(BF)
        for k in range(each):
            ref, place = places[c * each + k]
            for i in range(SLOTS):
                start = i * peers + k * UNIT
                ref[place, i * BLOCK : (i + 1) * BLOCK] = rows[start : start + UNIT, :]


def by_unit(rows, body):
    def step(k, carry):
        body(pl.multiple_of(k * UNIT, UNIT))
        return carry

    lax.fori_loop(0, rows // UNIT, step, 0)


def copy_rows(out_ref, out_start, in_ref, in_start, rows):
    def body(start):
        out_ref[pl.ds(out_start + start, UNIT), :] = in_ref[pl.ds(in_start + start, UNIT), :]

    by_unit(rows, body)


def unpack_rows_kernel(in_ref, low_ref, high_ref, both_ref):
    unpack(in_ref, low_ref, high_ref)
    half = low_ref.shape[0]
    copy_rows(both_ref, 0, low_ref, 0, half)
    copy_rows(both_ref, half, high_ref, 0, half)


def repack_rows_kernel(low_ref, high_ref, core_ref, *refs):
    *chips, out_ref, turned = refs
    size = out_ref.shape[0]
    peers = size // SLOTS
    each = peers // UNIT
    sources = [(low_ref, high_ref), (core_ref,), chips[0::2], chips[1::2]]
    for u, parts in enumerate(zip(*map(units, sources))):
        total = sum(ref[place, :].astype(F32) for ref, place in parts).astype(BF)
        c, start = u // each, u % each * UNIT
        for i in range(SLOTS):
            turned[i * peers + start : i * peers + start + UNIT, c * BLOCK : (c + 1) * BLOCK] = (
                total[:, i * BLOCK : (i + 1) * BLOCK]
            )
    out_ref[...] = dot(by_peer(size), turned[...]).astype(BF)


def add_kernel(own_ref, core_ref, *refs, first):
    *more, out_ref = refs

    def body(start):
        place = pl.ds(start, UNIT)
        total = own_ref[place, :].astype(F32) + core_ref[pl.ds(first + start, UNIT), :].astype(F32)
        for ref in more:
            total = total + ref[place, :].astype(F32)
        out_ref[place, :] = total.astype(BF)

    by_unit(own_ref.shape[0], body)


def add(own, core, second, *more):
    return vmem_call(
        lambda *refs: add_kernel(*refs, first=own.shape[0] * second),
        jax.ShapeDtypeStruct(own.shape, BF),
    )(own, core, *more)


def route_rows_kernel(slot_ref, weight_ref, high_ref, low_ref):
    slot = slot_of_row(high_ref.shape, 1, high_ref.shape[1] // USED)
    weight = sum(
        jnp.where(slot == slot_ref[:, k : k + 1], weight_ref[:, k : k + 1], 0.0) for k in (0, 1)
    )
    high = weight.astype(BF)
    high_ref[...] = high
    low_ref[...] = (weight - high.astype(F32)).astype(BF)


def combine_kernel(rows_ref, hidden_ref, high_ref, low_ref, out_ref, rows):
    unpack(rows_ref, rows)
    for i in range(SLOTS):
        columns = slice(i * BLOCK, (i + 1) * BLOCK)
        block = rows[:, columns]
        got = dot(high_ref[...], block) + dot(low_ref[...], block)
        out_ref[:, columns] = (hidden_ref[:, columns].astype(F32) + got).astype(BF)


def expert_kernel(*refs, count):
    parts = refs[:count]
    gate_ref, up_ref, down_ref = refs[count : count + 3]
    outs = refs[count + 3 : -2]
    rows, total = refs[-2:]
    step = pl.program_id(0)

    def starts(pieces):
        start = 0
        for piece in pieces:
            yield start
            start += piece.shape[0]

    @pl.when(step == 0)
    def _():
        for part, start in zip(parts, starts(parts)):
            copy_rows(rows, start, part, 0, part.shape[0])

    tile = rows.shape[0] // 2
    last = step == pl.num_programs(0) - 1

    def one_tile(k, carry):
        place = pl.ds(k * tile, tile)
        x = rows[place, :]
        hidden = (jax.nn.silu(dot(x, gate_ref[0])) * dot(x, up_ref[0])).astype(BF)
        piece = dot(hidden, down_ref[0])

        @pl.when(step == 0)
        def _():
            total[place, :] = piece

        @pl.when(last)
        def _():
            rows[place, :] = (total[place, :] + piece).astype(BF)

        return carry

    lax.fori_loop(0, 2, one_tile, 0)

    @pl.when(last)
    def _():
        for out, start in zip(outs, starts(outs)):
            copy_rows(out, 0, rows, start, out.shape[0])


def expert(parts, gate, up, down):
    count = len(parts)
    height = sum(part.shape[0] for part in parts)
    width = parts[0].shape[1]
    chunk = gate.shape[2] // 2
    outs = [parts[0].shape, parts[1].shape, (height // 2, width)]

    return pl.pallas_call(
        lambda *refs: expert_kernel(*refs, count=count),
        grid=(2,),
        in_specs=[whole(part.shape) for part in parts]
        + [
            pl.BlockSpec((1, width, chunk), lambda j: (0, 0, j)),
            pl.BlockSpec((1, width, chunk), lambda j: (0, 0, j)),
            pl.BlockSpec((1, chunk, width), lambda j: (0, j, 0)),
        ],
        out_specs=[whole(out) for out in outs],
        out_shape=[jax.ShapeDtypeStruct(out, BF) for out in outs],
        scratch_shapes=[pltpu.VMEM((height, width), BF), pltpu.VMEM((height, width), F32)],
        compiler_params=pltpu.CompilerParams(
            dimension_semantics=("arbitrary",), vmem_limit_bytes=20 * 1024 * 1024
        ),
        cost_estimate=pl.CostEstimate(
            flops=6 * height * width * gate.shape[2],
            bytes_accessed=2 * (2 * height * width + 3 * width * gate.shape[2]),
            transcendentals=height * gate.shape[2],
        ),
    )(*parts, gate, up, down)


def shift(a, where):
    return lax.ppermute(a, "tp", where)


def routed_experts(low, high, both, gate, up, down):
    def run(*parts):
        return expert(parts, gate, up, down)

    below_low, above_high = shift(low, UP), shift(high, DOWN)
    other = shift(both, OTHER_CORE)
    below_high, above_low = shift(high, UP), shift(low, DOWN)
    own_low, own_high, own = run(low, high, other)
    far_low, far_high = shift(below_low, UP), shift(above_high, DOWN)

    def both_cores(a, b):
        fetched = [shift(c, OTHER_CORE) for c in (a, b)]
        out_a, out_b, others = run(a, b, *fetched)
        back = shift(others, OTHER_CORE)
        return (out_a, back, 0), (out_b, back, 1)

    first = both_cores(below_low, above_high)
    second = both_cores(below_high, above_low)
    far = both_cores(far_low, far_high)
    from_above_low = shift(add(*first[0]), DOWN)
    from_below_high = shift(add(*first[1]), UP)
    to_above_low = shift(add(*far[0]), UP)
    to_below_high = shift(add(*far[1]), DOWN)
    from_above_high = shift(add(*second[0], to_below_high), DOWN)
    from_below_low = shift(add(*second[1], to_above_low), UP)
    own_back = shift(own, OTHER_CORE)
    return (
        own_low,
        own_high,
        own_back,
        from_below_low,
        from_above_low,
        from_below_high,
        from_above_high,
    )


STATE = 136


def write_state(out_ref, total, state):
    high = total.astype(BF).astype(F32)
    row = lax.broadcasted_iota(jnp.int32, (8, state.shape[1]), 0)
    line = jnp.where(row == 0, high, jnp.where(row == 1, total - high, 0.0))
    message = jnp.concatenate([state, line], axis=0).astype(BF)
    for k in range(out_ref.shape[0]):
        out_ref[k] = message


def read_states(ref):
    size = ref.shape[2]
    states = [ref[k, :size, :].astype(F32) for k in range(ref.shape[0])]
    lines = [ref[k, size:, :].astype(F32) for k in range(ref.shape[0])]
    return [line[0:1, :] + line[1:2, :] for line in lines], states


def weighted(totals, states, end):
    result = jnp.zeros_like(states[0])
    between = jnp.zeros_like(totals[0])
    for k in reversed(range(len(states))):
        result = result + jnp.where(k < end, jnp.exp(between), 0.0) * states[k]
        between = between + jnp.where(k < end, totals[k], 0.0)
    return result, between


def rotate(ref, cos_ref, sin_ref):
    rows = ref[...].astype(F32)
    return rows * cos_ref[...] + pltpu.roll(rows, ref.shape[1] // 2, 1) * sin_ref[...]


def block_state_kernel(
    key_ref, value_ref, decay_ref, cos_ref, sin_ref, row_ref, column_ref, out_ref, ready
):
    ready()
    width = key_ref.shape[1]
    blocks = decay_ref.shape[1] // width
    decay = jnp.concatenate(
        [decay_ref[:, k * width : (k + 1) * width] for k in range(blocks)]
        + [jnp.zeros((-blocks % 8, width), F32)],
        axis=0,
    )
    blocks = decay.shape[0]
    high = decay.astype(BF).astype(F32)
    middle = (decay - high).astype(BF).astype(F32)
    words = jnp.concatenate([high, middle, decay - high - middle], axis=0).astype(BF)
    upper = onehot(
        lax.broadcasted_iota(jnp.int32, (width, width), 0)
        <= lax.broadcasted_iota(jnp.int32, (width, width), 1)
    )
    sums = dot(words, upper)
    sums = sums[:blocks] + sums[blocks : 2 * blocks] + sums[2 * blocks :]
    total = jnp.zeros((1, 1), F32)
    rows = []
    for k in range(row_ref.shape[1] // width):
        rows.append(sums[k : k + 1, :] + total)
        total = rows[-1][:, width - 1 :]
    row_ref[...] = jnp.concatenate(rows, axis=1)
    column = jnp.concatenate([jnp.broadcast_to(r, (width, width)).T for r in rows], axis=0)
    column_ref[...] = column
    rotated = rotate(key_ref, cos_ref, sin_ref).astype(BF)
    damped = (rotated.astype(F32) * jnp.exp(total - column)).astype(BF)
    state = lax.dot_general(
        damped, value_ref[...], (((0,), (0,)), ((), ())), preferred_element_type=F32
    )
    write_state(out_ref, total, state)


def chip_row_kernel(in_ref, index_ref, inside_ref, ahead_ref, out_ref):
    totals, states = read_states(in_ref)
    inside, ahead = weighted(totals, states, index_ref[...])
    inside_ref[...] = inside
    ahead_ref[...] = ahead
    state, total = weighted(totals, states, len(states))
    write_state(out_ref, total, state)


def within_kernel(
    query_ref, key_ref, value_ref, row_ref, column_ref, cos_ref, sin_ref, turned_ref, out_ref, rotated
):
    width = query_ref.shape[1]
    turned_ref[...] = (rotate(query_ref, cos_ref, sin_ref) * width**-0.5).astype(BF)
    rotated[...] = rotate(key_ref, cos_ref, sin_ref).astype(BF)
    step = 256

    def some_rows(k, carry):
        place = pl.ds(k * step, step)
        scores = lax.dot_general(
            turned_ref[place, :],
            rotated[...],
            (((1,), (1,)), ((), ())),
            preferred_element_type=F32,
        )
        i = lax.broadcasted_iota(jnp.int32, scores.shape, 0) + k * step
        causal = i >= lax.broadcasted_iota(jnp.int32, scores.shape, 1)
        spread = column_ref[place, 0:1] - row_ref[...]
        decays = jnp.where(causal, jnp.exp(jnp.where(causal, spread, 0.0)), 0.0)
        out_ref[place, :] = dot((scores * decays).astype(BF), value_ref[...])
        return carry

    lax.fori_loop(0, query_ref.shape[0] // step, some_rows, 0)


def mix_kernel(
    in_ref, index_ref, inside_ref, ahead_ref, turned_ref, within_ref, column_ref, gate_ref, gain_ref, out_ref, ready
):
    totals, states = read_states(in_ref)
    before, _ = weighted(totals, states, index_ref[...])
    carried = jnp.exp(ahead_ref[...]) * before + inside_ref[...]
    high = carried.astype(BF)
    low = (carried - high.astype(F32)).astype(BF)
    ready()
    turned = turned_ref[...]
    readout = dot(turned, high) + dot(turned, low)
    out = within_ref[...] + jnp.exp(column_ref[...]) * readout
    scale = lax.rsqrt(jnp.mean(out * out, axis=1, keepdims=True) + epsilon)
    gate = gate_ref[...].astype(F32)
    out_ref[...] = (out * scale * gain_ref[...] * jax.nn.silu(gate)).astype(BF)


def slot_indices(route_ids, experts):
    flat_ids = route_ids.reshape(-1)
    chosen = (flat_ids[:, None] == jnp.arange(experts, dtype=jnp.int32)[None, :]).astype(jnp.int32)
    before = jnp.cumsum(chosen, axis=0) - chosen
    rank_in = jnp.sum(before * chosen, axis=1)
    return (flat_ids * SLOTS + rank_in).reshape(route_ids.shape)


def layer(
    residual,
    queries,
    key_rows,
    value_rows,
    gate_rows,
    log_decay,
    out_gain,
    out_weight,
    norm_gain,
    expert_gate,
    expert_up,
    expert_down,
    routes,
    route_weight,
):
    length, head_dim = queries.shape
    sp_count = lax.axis_size(SP)
    tp = lax.axis_index("tp")
    tp_count = lax.axis_size("tp")
    positions = (lax.axis_index(SP) * length + jnp.arange(length, dtype=jnp.int32)).astype(F32)
    column = jnp.arange(head_dim)
    half_dim = head_dim // 2
    inverse = rope_base ** (-(2 * (column % half_dim)).astype(F32) / head_dim)
    angles = positions[:, None] * inverse[None, :]
    cosine = jnp.cos(angles)
    sine = jnp.sin(angles) * jnp.where(column < half_dim, -1.0, 1.0)[None, :]
    shape = jax.ShapeDtypeStruct
    decay_row, decay_column, message = vmem_call(
        block_state_kernel,
        [
            shape((1, length), F32),
            shape((length, head_dim), F32),
            shape((lax.axis_size("sp_1"), STATE, head_dim), BF),
        ],
        late=(0, 1, 2),
    )(key_rows, value_rows, log_decay, cosine, sine)
    pieces = lax.all_to_all(message, "sp_1", 0, 0, tiled=True)
    rotated_queries, within = vmem_call(
        within_kernel,
        [shape((length, head_dim), BF), shape((length, head_dim), F32)],
        scratch_shapes=[pltpu.VMEM((length, head_dim), BF)],
        cost_estimate=pl.CostEstimate(
            flops=3 * length * length * head_dim,
            bytes_accessed=12 * length * head_dim,
            transcendentals=length * length,
        ),
    )(queries, key_rows, value_rows, decay_row, decay_column, cosine, sine)

    def index_line(axis):
        return jnp.full((1, head_dim), lax.axis_index(axis), jnp.int32)

    inside, ahead, message = vmem_call(
        chip_row_kernel,
        [
            shape((head_dim, head_dim), F32),
            shape((1, head_dim), F32),
            shape((lax.axis_size("sp_0"), STATE, head_dim), BF),
        ],
    )(pieces, index_line("sp_1"))
    pieces = lax.all_to_all(message, "sp_0", 0, 0, tiled=True)
    mixed = vmem_call(mix_kernel, shape((length, head_dim), BF), late=(4, 5, 7))(
        pieces,
        index_line("sp_0"),
        inside,
        ahead,
        rotated_queries,
        within,
        decay_column,
        gate_rows,
        out_gain[None],
    )

    weights = [
        out_weight, shift(out_weight, DOWN), shift(out_weight, ACROSS), shift(out_weight, UP)
    ]
    weights = weights + [shift(w, OTHER_CORE) for w in weights]

    row_count, model_width = residual.shape
    heads = lax.all_to_all(
        mixed.reshape(tp_count, row_count, head_dim), "tp", 0, 0, tiled=True
    )
    chip, core = tp // 2, tp % 2
    turned = lax.dynamic_slice_in_dim(jnp.concatenate([heads, heads]), 2 * chip, tp_count, 0)
    turned = turned.reshape(tp_count // 2, 2, row_count, head_dim)
    mine = jnp.where(core == 0, turned[:, 0], turned[:, 1])
    others = jnp.where(core == 0, turned[:, 1], turned[:, 0])

    slots = slot_indices(routes, sp_count)
    size = sp_count * SLOTS
    packed = shape((size, USED * BLOCK), BF)
    message = (sp_count, SLOTS, USED * BLOCK)
    turning = [pltpu.VMEM(packed.shape, BF)]
    hidden_res, tokens = vmem_call(
        project_and_pack_kernel,
        [shape((row_count, model_width), BF), packed],
        late=(10,),
        scratch_shapes=turning,
    )(mine, others, *weights, residual, norm_gain[None], slots.T)
    landed = lax.all_to_all(tokens.reshape(message), SP, 0, 0, tiled=True)
    half = shape((sp_count * USED // 2, model_width), BF)
    rows = vmem_call(
        unpack_rows_kernel, [half, half, shape((sp_count * USED, model_width), BF)]
    )(landed.reshape(packed.shape))
    route = shape((row_count, sp_count * USED), BF)
    high_weight, low_weight = vmem_call(route_rows_kernel, [route, route])(slots, route_weight)
    parts = routed_experts(*rows, expert_gate, expert_up, expert_down)
    repacked = vmem_call(repack_rows_kernel, packed, scratch_shapes=turning)(*parts)
    returned = lax.all_to_all(repacked.reshape(message), SP, 0, 0, tiled=True)
    return vmem_call(
        combine_kernel,
        shape(residual.shape, BF),
        scratch_shapes=[pltpu.VMEM((sp_count * USED, model_width), BF)],
    )(returned.reshape(packed.shape), hidden_res, high_weight, low_weight)


def solution(mesh):
    split = Mesh(mesh.devices.reshape(8, 4, mesh.shape["tp"]), ("sp_0", "sp_1", "tp"))
    in_specs = (
        P(SP_TP, None),
        P(SP, "tp"),
        P(SP, "tp"),
        P(SP, "tp"),
        P(SP, "tp"),
        P("tp", SP),
        P("tp"),
        P("tp", None),
        P(),
        P(SP, None, "tp"),
        P(SP, None, "tp"),
        P(SP, "tp", None),
        P(SP_TP, None),
        P(SP_TP, None),
    )
    out_specs = P(SP_TP, None)
    return jax.shard_map(layer, mesh=split, in_specs=in_specs, out_specs=out_specs, check_vma=False)
```

```python
import jax
import jax.numpy as jnp
from jax import lax
from jax.experimental import pallas as pl
from jax.experimental.pallas import tpu as pltpu
from jax.sharding import Mesh
from jax.sharding import PartitionSpec as P


SP = ("sp_0", "sp_1")
SP_TP = ("sp_0", "sp_1", "tp")


epsilon = 1e-06
rope_base = 10000.0
BF = jnp.bfloat16
F32 = jnp.float32

OTHER_CORE = [(i, i ^ 1) for i in range(8)]
UP = [(i, (i + 2) % 8) for i in range(8)]
DOWN = [(i, (i - 2) % 8) for i in range(8)]
ACROSS = [(i, (i + 4) % 8) for i in range(8)]

SLOTS = 8
USED = 7
UNIT = 16
BLOCK = 256
EARLY = 64


def dot(a, b):
    return jnp.dot(a, b, preferred_element_type=F32)


def whole(shape):
    return pl.BlockSpec(shape, lambda j: (0,) * len(shape))


def vmem_call(kernel, out_shape, late=(), scratch_shapes=(), **kwargs):
    def call(*args):
        args = [
            pltpu.with_memory_space_constraint(a, pltpu.HBM) if k in late else a
            for k, a in enumerate(args)
        ]
        count = len(args)
        outs = len(jax.tree.leaves(out_shape))
        buffers = [pltpu.VMEM(args[k].shape, args[k].dtype) for k in late]
        signals = [pltpu.SemaphoreType.DMA(())] * len(late)

        def body(*refs):
            ins = list(refs[:count])
            rest = refs[count : count + outs + len(scratch_shapes)]
            extra = refs[count + outs + len(scratch_shapes) :]
            copies = []
            for n, k in enumerate(late):
                copies.append(pltpu.make_async_copy(ins[k], extra[n], extra[len(late) + n]))
                copies[-1].start()
                ins[k] = extra[n]

            def ready():
                for copy in copies:
                    copy.wait()

            if late:
                kernel(*ins, *rest, ready=ready)
            else:
                kernel(*ins, *rest)

        return pl.pallas_call(
            body,
            in_specs=[
                pl.BlockSpec(memory_space=pltpu.HBM if k in late else pltpu.VMEM)
                for k in range(count)
            ],
            out_shape=out_shape,
            scratch_shapes=[*scratch_shapes, *buffers, *signals],
            compiler_params=pltpu.CompilerParams(vmem_limit_bytes=12 * 1024 * 1024),
            **kwargs,
        )(*args)

    return call


def onehot(mask):
    return jnp.where(mask, 1.0, 0.0).astype(BF)


def by_block(size):
    peers = size // SLOTS
    to = lax.broadcasted_iota(jnp.int32, (size, size), 0)
    source = lax.broadcasted_iota(jnp.int32, (size, size), 1)
    return onehot(source == (to & (peers - 1)) * SLOTS + to // peers)


def by_peer(size):
    peers = size // SLOTS
    to = lax.broadcasted_iota(jnp.int32, (size, size), 0)
    source = lax.broadcasted_iota(jnp.int32, (size, size), 1)
    return onehot(source == (to & 7) * peers + to // SLOTS)


def slot_of_row(shape, dim, peers):
    row = lax.broadcasted_iota(jnp.int32, shape, dim)
    return (row & (peers - 1)) * SLOTS + row // peers


def project_and_pack_kernel(*refs, ready):
    mine_ref, others_ref = refs[:2]
    weights = refs[2:10]
    residual_ref, gain_ref, slot_ref, hidden_ref, out_ref, turned = refs[10:]
    tokens, width = residual_ref.shape
    size = out_ref.shape[0]
    peers = size // SLOTS
    heads = jnp.concatenate([ref[k] for ref in (mine_ref, others_ref) for k in range(4)], axis=1)
    squares = jnp.zeros((tokens, 1), F32)
    step = 512
    for start in range(0, width, step):
        columns = slice(start, start + step)
        projected = dot(heads, jnp.concatenate([w[:, columns] for w in weights], axis=0))
        if start == 0:
            ready()
        hidden = (residual_ref[:, columns].astype(F32) + projected).astype(BF)
        hidden_ref[:, columns] = hidden
        hidden_f = hidden.astype(F32)
        squares = squares + jnp.sum(hidden_f * hidden_f, axis=1, keepdims=True)
    scale = lax.rsqrt(squares / width + epsilon)
    slot = slot_of_row((USED * peers, tokens), 0, peers)
    chosen = onehot((slot == slot_ref[0:1, :]) | (slot == slot_ref[1:2, :]))
    for i in range(SLOTS):
        columns = slice(i * BLOCK, (i + 1) * BLOCK)
        normed = hidden_ref[:, columns].astype(F32) * scale * gain_ref[:, columns]
        picked = dot(chosen, normed.astype(BF)).astype(BF)
        for c in range(USED):
            turned[i * peers : (i + 1) * peers, c * BLOCK : (c + 1) * BLOCK] = picked[
                c * peers : (c + 1) * peers, :
            ]
    out_ref[...] = dot(by_peer(size), turned[...]).astype(BF)


def units(refs):
    for ref in refs:
        for start in range(0, ref.shape[0], UNIT):
            yield ref, slice(start, start + UNIT)


def unpack(in_ref, *out_refs):
    size = in_ref.shape[0]
    peers = size // SLOTS
    order = by_block(size)
    places = list(units(out_refs))
    each = peers // UNIT
    for c in range(in_ref.shape[1] // BLOCK):
        rows = dot(order, in_ref[:, c * BLOCK : (c + 1) * BLOCK]).astype(BF)
        for k in range(each):
            ref, place = places[c * each + k]
            for i in range(SLOTS):
                start = i * peers + k * UNIT
                ref[place, i * BLOCK : (i + 1) * BLOCK] = rows[start : start + UNIT, :]


def by_unit(rows, body):
    def step(k, carry):
        body(pl.multiple_of(k * UNIT, UNIT))
        return carry

    lax.fori_loop(0, rows // UNIT, step, 0)


def copy_rows(out_ref, out_start, in_ref, in_start, rows):
    def body(start):
        out_ref[pl.ds(out_start + start, UNIT), :] = in_ref[pl.ds(in_start + start, UNIT), :]

    by_unit(rows, body)


def unpack_rows_kernel(in_ref, low_ref, high_ref, both_ref):
    unpack(in_ref, low_ref, high_ref)
    half = low_ref.shape[0]
    copy_rows(both_ref, 0, low_ref, 0, half)
    copy_rows(both_ref, half, high_ref, 0, half)


def repack_rows_kernel(*refs, counts):
    out_ref, turned = refs[-2:]
    size = out_ref.shape[0]
    peers = size // SLOTS
    each = peers // UNIT
    sources, start = [], 0
    for count in counts:
        sources.append(refs[start : start + count])
        start += count
    for u, parts in enumerate(zip(*map(units, sources))):
        total = sum(ref[place, :].astype(F32) for ref, place in parts).astype(BF)
        c, start = u // each, u % each * UNIT
        for i in range(SLOTS):
            turned[i * peers + start : i * peers + start + UNIT, c * BLOCK : (c + 1) * BLOCK] = (
                total[:, i * BLOCK : (i + 1) * BLOCK]
            )
    out_ref[...] = dot(by_peer(size), turned[...]).astype(BF)


def add_kernel(*refs, windows):
    outs = refs[-len(windows) :]
    for (own, core, more, own_first, core_first), out_ref in zip(windows, outs):

        def body(start):
            total = refs[own][pl.ds(own_first + start, UNIT), :].astype(F32)
            total = total + refs[core][pl.ds(core_first + start, UNIT), :].astype(F32)
            if more is not None:
                total = total + refs[more][pl.ds(start, UNIT), :].astype(F32)
            out_ref[pl.ds(start, UNIT), :] = total.astype(BF)

        by_unit(out_ref.shape[0], body)


def add(own, core, second, more, first, rows):
    windows = [(0, 1, 2, first, own.shape[0] * second + first)]
    return vmem_call(
        lambda *refs: add_kernel(*refs, windows=windows),
        [jax.ShapeDtypeStruct((rows, own.shape[1]), BF)],
    )(own, core, more)[0]


def add_both(a, b, core, pieces, skip=0):
    rows, width = a.shape
    windows = [
        (half, 2, None, first, skip + rows * half + first) for half in (0, 1) for first, _ in pieces
    ]
    return vmem_call(
        lambda *refs: add_kernel(*refs, windows=windows),
        [jax.ShapeDtypeStruct((count, width), BF) for _ in (0, 1) for _, count in pieces],
    )(a, b, core)


def route_rows_kernel(slot_ref, weight_ref, high_ref, low_ref):
    slot = slot_of_row(high_ref.shape, 1, high_ref.shape[1] // USED)
    weight = sum(
        jnp.where(slot == slot_ref[:, k : k + 1], weight_ref[:, k : k + 1], 0.0) for k in (0, 1)
    )
    high = weight.astype(BF)
    high_ref[...] = high
    low_ref[...] = (weight - high.astype(F32)).astype(BF)


def combine_kernel(rows_ref, hidden_ref, high_ref, low_ref, out_ref, rows):
    unpack(rows_ref, rows)
    for i in range(SLOTS):
        columns = slice(i * BLOCK, (i + 1) * BLOCK)
        block = rows[:, columns]
        got = dot(high_ref[...], block) + dot(low_ref[...], block)
        out_ref[:, columns] = (hidden_ref[:, columns].astype(F32) + got).astype(BF)


def expert_kernel(*refs, count, tiles):
    parts = refs[:count]
    gate_ref, up_ref, down_ref = refs[count : count + 3]
    outs = refs[count + 3 : -2]
    rows, total = refs[-2:]
    step = pl.program_id(0)

    def starts(pieces):
        start = 0
        for piece in pieces:
            yield start
            start += piece.shape[0]

    @pl.when(step == 0)
    def _():
        for part, start in zip(parts, starts(parts)):
            copy_rows(rows, start, part, 0, part.shape[0])

    tile = rows.shape[0] // tiles
    last = step == pl.num_programs(0) - 1

    def one_tile(k, carry):
        place = pl.ds(k * tile, tile)
        x = rows[place, :]
        hidden = (jax.nn.silu(dot(x, gate_ref[0])) * dot(x, up_ref[0])).astype(BF)
        piece = dot(hidden, down_ref[0])

        @pl.when(step == 0)
        def _():
            total[place, :] = piece

        @pl.when(last)
        def _():
            rows[place, :] = (total[place, :] + piece).astype(BF)

        return carry

    lax.fori_loop(0, tiles, one_tile, 0)

    @pl.when(last)
    def _():
        for out, start in zip(outs, starts(outs)):
            copy_rows(out, 0, rows, start, out.shape[0])


def expert(own, fetched, gate, up, down, tiles):
    parts = (*own, *fetched)
    count = len(parts)
    height = sum(part.shape[0] for part in parts)
    width = parts[0].shape[1]
    chunk = gate.shape[2] // 2
    outs = [part.shape for part in own] + [(height // 2, width)]

    return pl.pallas_call(
        lambda *refs: expert_kernel(*refs, count=count, tiles=tiles),
        grid=(2,),
        in_specs=[whole(part.shape) for part in parts]
        + [
            pl.BlockSpec((1, width, chunk), lambda j: (0, 0, j)),
            pl.BlockSpec((1, width, chunk), lambda j: (0, 0, j)),
            pl.BlockSpec((1, chunk, width), lambda j: (0, j, 0)),
        ],
        out_specs=[whole(out) for out in outs],
        out_shape=[jax.ShapeDtypeStruct(out, BF) for out in outs],
        scratch_shapes=[pltpu.VMEM((height, width), BF), pltpu.VMEM((height, width), F32)],
        compiler_params=pltpu.CompilerParams(
            dimension_semantics=("arbitrary",), vmem_limit_bytes=20 * 1024 * 1024
        ),
        cost_estimate=pl.CostEstimate(
            flops=6 * height * width * gate.shape[2],
            bytes_accessed=2 * (2 * height * width + 3 * width * gate.shape[2]),
            transcendentals=height * gate.shape[2],
        ),
    )(*parts, gate, up, down)


def shift(a, where):
    return lax.ppermute(a, "tp", where)


def routed_experts(low, high, both, gate, up, down):
    def both_cores(own, *fetched, tiles):
        *outs, others = expert(own, fetched, gate, up, down, tiles)
        return *outs, shift(others, OTHER_CORE)

    def swap(*parts):
        return [shift(part, OTHER_CORE) for part in parts]

    below_low, above_high = shift(low, UP), shift(high, DOWN)
    other = shift(both, OTHER_CORE)
    below_high, above_low = shift(high, UP), shift(low, DOWN)
    far_low, far_high = shift(below_low, UP), shift(above_high, DOWN)
    near = (below_low, above_high)
    own_low, own_high, *first = both_cores((low, high, *near), other, *swap(*near), tiles=8)
    late = (below_high, above_low)
    second = both_cores(late, *swap(*late), tiles=4)
    ends = (far_low, far_high)
    far = both_cores(ends, *swap(*ends), tiles=2)
    rows = low.shape[0]
    pieces = ((0, EARLY), (EARLY, rows - EARLY))
    to_below, to_above = add_both(*first, ((0, rows),), skip=2 * rows)
    from_above_low, from_below_high = shift(to_below, DOWN), shift(to_above, UP)
    to_far = add_both(*far, pieces)
    from_below_low, from_above_high = [], []
    for k, window in enumerate(pieces):
        ups, downs = shift(to_far[k], UP), shift(to_far[2 + k], DOWN)
        ups = add(second[1], second[2], 1, ups, *window)
        downs = add(second[0], second[2], 0, downs, *window)
        from_below_low.append(shift(ups, UP))
        from_above_high.append(shift(downs, DOWN))
    return (
        (own_low, own_high),
        (first[2],),
        (*from_below_low, from_below_high),
        (from_above_low, *from_above_high),
    )


STATE = 136


def write_state(out_ref, total, state):
    high = total.astype(BF).astype(F32)
    row = lax.broadcasted_iota(jnp.int32, (8, state.shape[1]), 0)
    line = jnp.where(row == 0, high, jnp.where(row == 1, total - high, 0.0))
    message = jnp.concatenate([state, line], axis=0).astype(BF)
    for k in range(out_ref.shape[0]):
        out_ref[k] = message


def read_states(ref):
    size = ref.shape[2]
    states = [ref[k, :size, :].astype(F32) for k in range(ref.shape[0])]
    lines = [ref[k, size:, :].astype(F32) for k in range(ref.shape[0])]
    return [line[0:1, :] + line[1:2, :] for line in lines], states


def weighted(totals, states, end):
    result = jnp.zeros_like(states[0])
    between = jnp.zeros_like(totals[0])
    for k in reversed(range(len(states))):
        result = result + jnp.where(k < end, jnp.exp(between), 0.0) * states[k]
        between = between + jnp.where(k < end, totals[k], 0.0)
    return result, between


def rotate(ref, cos_ref, sin_ref):
    rows = ref[...].astype(F32)
    return rows * cos_ref[...] + pltpu.roll(rows, ref.shape[1] // 2, 1) * sin_ref[...]


def block_state_kernel(
    key_ref, value_ref, decay_ref, cos_ref, sin_ref, row_ref, column_ref, out_ref, ready
):
    ready()
    width = key_ref.shape[1]
    blocks = decay_ref.shape[1] // width
    decay = jnp.concatenate(
        [decay_ref[:, k * width : (k + 1) * width] for k in range(blocks)]
        + [jnp.zeros((-blocks % 8, width), F32)],
        axis=0,
    )
    blocks = decay.shape[0]
    high = decay.astype(BF).astype(F32)
    middle = (decay - high).astype(BF).astype(F32)
    words = jnp.concatenate([high, middle, decay - high - middle], axis=0).astype(BF)
    upper = onehot(
        lax.broadcasted_iota(jnp.int32, (width, width), 0)
        <= lax.broadcasted_iota(jnp.int32, (width, width), 1)
    )
    sums = dot(words, upper)
    sums = sums[:blocks] + sums[blocks : 2 * blocks] + sums[2 * blocks :]
    total = jnp.zeros((1, 1), F32)
    rows = []
    for k in range(row_ref.shape[1] // width):
        rows.append(sums[k : k + 1, :] + total)
        total = rows[-1][:, width - 1 :]
    row_ref[...] = jnp.concatenate(rows, axis=1)
    column = jnp.concatenate([jnp.broadcast_to(r, (width, width)).T for r in rows], axis=0)
    column_ref[...] = column
    rotated = rotate(key_ref, cos_ref, sin_ref).astype(BF)
    damped = (rotated.astype(F32) * jnp.exp(total - column)).astype(BF)
    state = lax.dot_general(
        damped, value_ref[...], (((0,), (0,)), ((), ())), preferred_element_type=F32
    )
    write_state(out_ref, total, state)


def chip_row_kernel(in_ref, index_ref, inside_ref, ahead_ref, out_ref):
    totals, states = read_states(in_ref)
    inside, ahead = weighted(totals, states, index_ref[...])
    inside_ref[...] = inside
    ahead_ref[...] = ahead
    state, total = weighted(totals, states, len(states))
    write_state(out_ref, total, state)


def within_kernel(
    query_ref, key_ref, value_ref, row_ref, column_ref, cos_ref, sin_ref, turned_ref, out_ref, rotated
):
    width = query_ref.shape[1]
    turned_ref[...] = (rotate(query_ref, cos_ref, sin_ref) * width**-0.5).astype(BF)
    rotated[...] = rotate(key_ref, cos_ref, sin_ref).astype(BF)
    step = 256

    def some_rows(k, carry):
        place = pl.ds(k * step, step)
        scores = lax.dot_general(
            turned_ref[place, :],
            rotated[...],
            (((1,), (1,)), ((), ())),
            preferred_element_type=F32,
        )
        i = lax.broadcasted_iota(jnp.int32, scores.shape, 0) + k * step
        causal = i >= lax.broadcasted_iota(jnp.int32, scores.shape, 1)
        spread = column_ref[place, 0:1] - row_ref[...]
        decays = jnp.where(causal, jnp.exp(jnp.where(causal, spread, 0.0)), 0.0)
        out_ref[place, :] = dot((scores * decays).astype(BF), value_ref[...])
        return carry

    lax.fori_loop(0, query_ref.shape[0] // step, some_rows, 0)


def mix_kernel(
    in_ref, index_ref, inside_ref, ahead_ref, turned_ref, within_ref, column_ref, gate_ref, gain_ref, out_ref, ready
):
    totals, states = read_states(in_ref)
    before, _ = weighted(totals, states, index_ref[...])
    carried = jnp.exp(ahead_ref[...]) * before + inside_ref[...]
    high = carried.astype(BF)
    low = (carried - high.astype(F32)).astype(BF)
    ready()
    turned = turned_ref[...]
    readout = dot(turned, high) + dot(turned, low)
    out = within_ref[...] + jnp.exp(column_ref[...]) * readout
    scale = lax.rsqrt(jnp.mean(out * out, axis=1, keepdims=True) + epsilon)
    gate = gate_ref[...].astype(F32)
    out_ref[...] = (out * scale * gain_ref[...] * jax.nn.silu(gate)).astype(BF)


def slot_indices(route_ids, experts):
    flat_ids = route_ids.reshape(-1)
    chosen = (flat_ids[:, None] == jnp.arange(experts, dtype=jnp.int32)[None, :]).astype(jnp.int32)
    before = jnp.cumsum(chosen, axis=0) - chosen
    rank_in = jnp.sum(before * chosen, axis=1)
    return (flat_ids * SLOTS + rank_in).reshape(route_ids.shape)


def layer(
    residual,
    queries,
    key_rows,
    value_rows,
    gate_rows,
    log_decay,
    out_gain,
    out_weight,
    norm_gain,
    expert_gate,
    expert_up,
    expert_down,
    routes,
    route_weight,
):
    length, head_dim = queries.shape
    sp_count = lax.axis_size(SP)
    tp = lax.axis_index("tp")
    tp_count = lax.axis_size("tp")
    positions = (lax.axis_index(SP) * length + jnp.arange(length, dtype=jnp.int32)).astype(F32)
    column = jnp.arange(head_dim)
    half_dim = head_dim // 2
    inverse = rope_base ** (-(2 * (column % half_dim)).astype(F32) / head_dim)
    angles = positions[:, None] * inverse[None, :]
    cosine = jnp.cos(angles)
    sine = jnp.sin(angles) * jnp.where(column < half_dim, -1.0, 1.0)[None, :]
    shape = jax.ShapeDtypeStruct
    decay_row, decay_column, message = vmem_call(
        block_state_kernel,
        [
            shape((1, length), F32),
            shape((length, head_dim), F32),
            shape((lax.axis_size("sp_1"), STATE, head_dim), BF),
        ],
        late=(0, 1, 2),
    )(key_rows, value_rows, log_decay, cosine, sine)
    pieces = lax.all_to_all(message, "sp_1", 0, 0, tiled=True)
    rotated_queries, within = vmem_call(
        within_kernel,
        [shape((length, head_dim), BF), shape((length, head_dim), F32)],
        scratch_shapes=[pltpu.VMEM((length, head_dim), BF)],
        cost_estimate=pl.CostEstimate(
            flops=3 * length * length * head_dim,
            bytes_accessed=12 * length * head_dim,
            transcendentals=length * length,
        ),
    )(queries, key_rows, value_rows, decay_row, decay_column, cosine, sine)

    def index_line(axis):
        return jnp.full((1, head_dim), lax.axis_index(axis), jnp.int32)

    inside, ahead, message = vmem_call(
        chip_row_kernel,
        [
            shape((head_dim, head_dim), F32),
            shape((1, head_dim), F32),
            shape((lax.axis_size("sp_0"), STATE, head_dim), BF),
        ],
    )(pieces, index_line("sp_1"))
    pieces = lax.all_to_all(message, "sp_0", 0, 0, tiled=True)
    mixed = vmem_call(mix_kernel, shape((length, head_dim), BF), late=(4, 5, 7))(
        pieces,
        index_line("sp_0"),
        inside,
        ahead,
        rotated_queries,
        within,
        decay_column,
        gate_rows,
        out_gain[None],
    )

    weights = [
        out_weight, shift(out_weight, DOWN), shift(out_weight, ACROSS), shift(out_weight, UP)
    ]
    weights = weights + [shift(w, OTHER_CORE) for w in weights]

    row_count, model_width = residual.shape
    heads = lax.all_to_all(
        mixed.reshape(tp_count, row_count, head_dim), "tp", 0, 0, tiled=True
    )
    chip, core = tp // 2, tp % 2
    turned = lax.dynamic_slice_in_dim(jnp.concatenate([heads, heads]), 2 * chip, tp_count, 0)
    turned = turned.reshape(tp_count // 2, 2, row_count, head_dim)
    mine = jnp.where(core == 0, turned[:, 0], turned[:, 1])
    others = jnp.where(core == 0, turned[:, 1], turned[:, 0])

    slots = slot_indices(routes, sp_count)
    size = sp_count * SLOTS
    packed = shape((size, USED * BLOCK), BF)
    message = (sp_count, SLOTS, USED * BLOCK)
    turning = [pltpu.VMEM(packed.shape, BF)]
    hidden_res, tokens = vmem_call(
        project_and_pack_kernel,
        [shape((row_count, model_width), BF), packed],
        late=(10,),
        scratch_shapes=turning,
    )(mine, others, *weights, residual, norm_gain[None], slots.T)
    landed = lax.all_to_all(tokens.reshape(message), SP, 0, 0, tiled=True)
    half = shape((sp_count * USED // 2, model_width), BF)
    rows = vmem_call(
        unpack_rows_kernel, [half, half, shape((sp_count * USED, model_width), BF)]
    )(landed.reshape(packed.shape))
    route = shape((row_count, sp_count * USED), BF)
    high_weight, low_weight = vmem_call(route_rows_kernel, [route, route])(slots, route_weight)
    parts = routed_experts(*rows, expert_gate, expert_up, expert_down)
    counts = tuple(map(len, parts))
    repacked = vmem_call(
        lambda *refs: repack_rows_kernel(*refs, counts=counts), packed, scratch_shapes=turning
    )(*[ref for part in parts for ref in part])
    returned = lax.all_to_all(repacked.reshape(message), SP, 0, 0, tiled=True)
    return vmem_call(
        combine_kernel,
        shape(residual.shape, BF),
        scratch_shapes=[pltpu.VMEM((sp_count * USED, model_width), BF)],
    )(returned.reshape(packed.shape), hidden_res, high_weight, low_weight)


def solution(mesh):
    split = Mesh(mesh.devices.reshape(8, 4, mesh.shape["tp"]), ("sp_0", "sp_1", "tp"))
    in_specs = (
        P(SP_TP, None),
        P(SP, "tp"),
        P(SP, "tp"),
        P(SP, "tp"),
        P(SP, "tp"),
        P("tp", SP),
        P("tp"),
        P("tp", None),
        P(),
        P(SP, None, "tp"),
        P(SP, None, "tp"),
        P(SP, "tp", None),
        P(SP_TP, None),
        P(SP_TP, None),
    )
    out_specs = P(SP_TP, None)
    return jax.shard_map(layer, mesh=split, in_specs=in_specs, out_specs=out_specs, check_vma=False)
```

```python
import jax
import jax.numpy as jnp
from jax import lax
from jax.experimental import pallas as pl
from jax.experimental.pallas import tpu as pltpu
from jax.sharding import Mesh
from jax.sharding import PartitionSpec as P


SP = ("sp_0", "sp_1")
SP_TP = ("sp_0", "sp_1", "tp")


epsilon = 1e-06
rope_base = 10000.0
BF = jnp.bfloat16
F32 = jnp.float32

OTHER_CORE = [(i, i ^ 1) for i in range(8)]
UP = [(i, (i + 2) % 8) for i in range(8)]
DOWN = [(i, (i - 2) % 8) for i in range(8)]
ACROSS = [(i, (i + 4) % 8) for i in range(8)]

SLOTS = 8
USED = 7
UNIT = 16
BLOCK = 256
EARLY = 64


def dot(a, b):
    return jnp.dot(a, b, preferred_element_type=F32)


def whole(shape):
    return pl.BlockSpec(shape, lambda j: (0,) * len(shape))


def vmem_call(kernel, out_shape, late=(), scratch_shapes=(), **kwargs):
    def call(*args):
        args = [
            pltpu.with_memory_space_constraint(a, pltpu.HBM) if k in late else a
            for k, a in enumerate(args)
        ]
        count = len(args)
        outs = len(jax.tree.leaves(out_shape))
        buffers = [pltpu.VMEM(args[k].shape, args[k].dtype) for k in late]
        signals = [pltpu.SemaphoreType.DMA(())] * len(late)

        def body(*refs):
            ins = list(refs[:count])
            rest = refs[count : count + outs + len(scratch_shapes)]
            extra = refs[count + outs + len(scratch_shapes) :]
            copies = []
            for n, k in enumerate(late):
                copies.append(pltpu.make_async_copy(ins[k], extra[n], extra[len(late) + n]))
                copies[-1].start()
                ins[k] = extra[n]

            def ready():
                for copy in copies:
                    copy.wait()

            if late:
                kernel(*ins, *rest, ready=ready)
            else:
                kernel(*ins, *rest)

        return pl.pallas_call(
            body,
            in_specs=[
                pl.BlockSpec(memory_space=pltpu.HBM if k in late else pltpu.VMEM)
                for k in range(count)
            ],
            out_shape=out_shape,
            scratch_shapes=[*scratch_shapes, *buffers, *signals],
            compiler_params=pltpu.CompilerParams(vmem_limit_bytes=12 * 1024 * 1024),
            **kwargs,
        )(*args)

    return call


def onehot(mask):
    return jnp.where(mask, 1.0, 0.0).astype(BF)


def by_block(size):
    peers = size // SLOTS
    to = lax.broadcasted_iota(jnp.int32, (size, size), 0)
    source = lax.broadcasted_iota(jnp.int32, (size, size), 1)
    return onehot(source == (to & (peers - 1)) * SLOTS + to // peers)


def by_peer(size):
    peers = size // SLOTS
    to = lax.broadcasted_iota(jnp.int32, (size, size), 0)
    source = lax.broadcasted_iota(jnp.int32, (size, size), 1)
    return onehot(source == (to & 7) * peers + to // SLOTS)


def slot_of_row(shape, dim, peers):
    row = lax.broadcasted_iota(jnp.int32, shape, dim)
    return (row & (peers - 1)) * SLOTS + row // peers


def project_and_pack_kernel(*refs, ready):
    mine_ref, others_ref = refs[:2]
    weights = refs[2:10]
    residual_ref, gain_ref, slot_ref, hidden_ref, out_ref, turned = refs[10:]
    tokens, width = residual_ref.shape
    size = out_ref.shape[0]
    peers = size // SLOTS
    heads = jnp.concatenate([ref[k] for ref in (mine_ref, others_ref) for k in range(4)], axis=1)
    squares = jnp.zeros((tokens, 1), F32)
    step = 512
    for start in range(0, width, step):
        columns = slice(start, start + step)
        projected = dot(heads, jnp.concatenate([w[:, columns] for w in weights], axis=0))
        if start == 0:
            ready()
        hidden = (residual_ref[:, columns].astype(F32) + projected).astype(BF)
        hidden_ref[:, columns] = hidden
        hidden_f = hidden.astype(F32)
        squares = squares + jnp.sum(hidden_f * hidden_f, axis=1, keepdims=True)
    scale = lax.rsqrt(squares / width + epsilon)
    slot = slot_of_row((USED * peers, tokens), 0, peers)
    chosen = onehot((slot == slot_ref[0:1, :]) | (slot == slot_ref[1:2, :]))
    for i in range(SLOTS):
        columns = slice(i * BLOCK, (i + 1) * BLOCK)
        normed = hidden_ref[:, columns].astype(F32) * scale * gain_ref[:, columns]
        picked = dot(chosen, normed.astype(BF)).astype(BF)
        for c in range(USED):
            turned[i * peers : (i + 1) * peers, c * BLOCK : (c + 1) * BLOCK] = picked[
                c * peers : (c + 1) * peers, :
            ]
    out_ref[...] = dot(by_peer(size), turned[...]).astype(BF)


def units(refs):
    for ref in refs:
        for start in range(0, ref.shape[0], UNIT):
            yield ref, slice(start, start + UNIT)


def unpack(in_ref, *out_refs):
    size = in_ref.shape[0]
    peers = size // SLOTS
    order = by_block(size)
    places = list(units(out_refs))
    each = peers // UNIT
    for c in range(in_ref.shape[1] // BLOCK):
        rows = dot(order, in_ref[:, c * BLOCK : (c + 1) * BLOCK]).astype(BF)
        for k in range(each):
            ref, place = places[c * each + k]
            for i in range(SLOTS):
                start = i * peers + k * UNIT
                ref[place, i * BLOCK : (i + 1) * BLOCK] = rows[start : start + UNIT, :]


def by_unit(rows, body):
    def step(k, carry):
        body(pl.multiple_of(k * UNIT, UNIT))
        return carry

    lax.fori_loop(0, rows // UNIT, step, 0)


def copy_rows(out_ref, out_start, in_ref, in_start, rows):
    def body(start):
        out_ref[pl.ds(out_start + start, UNIT), :] = in_ref[pl.ds(in_start + start, UNIT), :]

    by_unit(rows, body)


def unpack_rows_kernel(in_ref, low_ref, high_ref, both_ref):
    unpack(in_ref, low_ref, high_ref)
    half = low_ref.shape[0]
    copy_rows(both_ref, 0, low_ref, 0, half)
    copy_rows(both_ref, half, high_ref, 0, half)


def repack_rows_kernel(*refs, counts):
    out_ref, turned = refs[-2:]
    size = out_ref.shape[0]
    peers = size // SLOTS
    each = peers // UNIT
    sources, start = [], 0
    for count in counts:
        sources.append(refs[start : start + count])
        start += count
    for u, parts in enumerate(zip(*map(units, sources))):
        total = sum(ref[place, :].astype(F32) for ref, place in parts).astype(BF)
        c, start = u // each, u % each * UNIT
        for i in range(SLOTS):
            turned[i * peers + start : i * peers + start + UNIT, c * BLOCK : (c + 1) * BLOCK] = (
                total[:, i * BLOCK : (i + 1) * BLOCK]
            )
    out_ref[...] = dot(by_peer(size), turned[...]).astype(BF)


def add_kernel(*refs, windows):
    outs = refs[-len(windows) :]
    for (own, core, more, own_first, core_first), out_ref in zip(windows, outs):

        def body(start):
            total = refs[own][pl.ds(own_first + start, UNIT), :].astype(F32)
            total = total + refs[core][pl.ds(core_first + start, UNIT), :].astype(F32)
            if more is not None:
                total = total + refs[more][pl.ds(start, UNIT), :].astype(F32)
            out_ref[pl.ds(start, UNIT), :] = total.astype(BF)

        by_unit(out_ref.shape[0], body)


def add(own, core, second, more, first, rows):
    windows = [(0, 1, 2, first, own.shape[0] * second + first)]
    return vmem_call(
        lambda *refs: add_kernel(*refs, windows=windows),
        [jax.ShapeDtypeStruct((rows, own.shape[1]), BF)],
    )(own, core, more)[0]


def add_both(a, b, core, pieces, skip=0):
    rows, width = a.shape
    windows = [
        (half, 2, None, first, skip + rows * half + first) for half in (0, 1) for first, _ in pieces
    ]
    return vmem_call(
        lambda *refs: add_kernel(*refs, windows=windows),
        [jax.ShapeDtypeStruct((count, width), BF) for _ in (0, 1) for _, count in pieces],
    )(a, b, core)


def route_rows_kernel(slot_ref, weight_ref, high_ref, low_ref):
    slot = slot_of_row(high_ref.shape, 1, high_ref.shape[1] // USED)
    weight = sum(
        jnp.where(slot == slot_ref[:, k : k + 1], weight_ref[:, k : k + 1], 0.0) for k in (0, 1)
    )
    high = weight.astype(BF)
    high_ref[...] = high
    low_ref[...] = (weight - high.astype(F32)).astype(BF)


def combine_kernel(rows_ref, hidden_ref, high_ref, low_ref, out_ref, rows):
    unpack(rows_ref, rows)
    for i in range(SLOTS):
        columns = slice(i * BLOCK, (i + 1) * BLOCK)
        block = rows[:, columns]
        got = dot(high_ref[...], block) + dot(low_ref[...], block)
        out_ref[:, columns] = (hidden_ref[:, columns].astype(F32) + got).astype(BF)


def expert_kernel(*refs, count, ready, tiles):
    parts = refs[:count]
    gate_ref, up_ref, down_ref = refs[count : count + 3]
    passed = refs[count + 3 : count + 3 + ready]
    outs = refs[count + 3 + ready : -2]
    rows, total = refs[-2:]
    step = pl.program_id(0)

    def starts(pieces):
        start = 0
        for piece in pieces:
            yield start
            start += piece.shape[0]

    @pl.when(step == 0)
    def _():
        for part, start in zip(parts, starts(parts)):
            copy_rows(rows, start, part, 0, part.shape[0])

    tile = rows.shape[0] // tiles
    last = step == pl.num_programs(0) - 1

    def one_tile(k, carry):
        place = pl.ds(k * tile, tile)
        x = rows[place, :]
        hidden = (jax.nn.silu(dot(x, gate_ref[0])) * dot(x, up_ref[0])).astype(BF)
        piece = dot(hidden, down_ref[0])

        @pl.when(step == 0)
        def _():
            total[place, :] = piece

        @pl.when(last)
        def _():
            rows[place, :] = (total[place, :] + piece).astype(BF)

        return carry

    lax.fori_loop(0, tiles, one_tile, 0)

    @pl.when(last)
    def _():
        ahead = 0
        for ref in passed:
            copy_rows(outs[-1], ahead, ref, 0, ref.shape[0])
            ahead += ref.shape[0]
        for out, start in zip(outs, starts(outs)):
            first = ahead if out is outs[-1] else 0
            copy_rows(out, first, rows, start, out.shape[0] - first)


def expert(own, fetched, ready, gate, up, down, tiles):
    parts = (*own, *fetched)
    count = len(parts)
    ahead = sum(part.shape[0] for part in ready)
    height = sum(part.shape[0] for part in parts)
    width = parts[0].shape[1]
    chunk = gate.shape[2] // 2
    outs = [part.shape for part in own] + [(ahead + height // 2, width)]

    return pl.pallas_call(
        lambda *refs: expert_kernel(*refs, count=count, ready=len(ready), tiles=tiles),
        grid=(2,),
        in_specs=[whole(part.shape) for part in parts]
        + [
            pl.BlockSpec((1, width, chunk), lambda j: (0, 0, j)),
            pl.BlockSpec((1, width, chunk), lambda j: (0, 0, j)),
            pl.BlockSpec((1, chunk, width), lambda j: (0, j, 0)),
        ]
        + [whole(part.shape) for part in ready],
        out_specs=[whole(out) for out in outs],
        out_shape=[jax.ShapeDtypeStruct(out, BF) for out in outs],
        scratch_shapes=[pltpu.VMEM((height, width), BF), pltpu.VMEM((height, width), F32)],
        compiler_params=pltpu.CompilerParams(
            dimension_semantics=("arbitrary",), vmem_limit_bytes=20 * 1024 * 1024
        ),
        cost_estimate=pl.CostEstimate(
            flops=6 * height * width * gate.shape[2],
            bytes_accessed=2 * (2 * height * width + 3 * width * gate.shape[2]),
            transcendentals=height * gate.shape[2],
        ),
    )(*parts, gate, up, down, *ready)


def shift(a, where):
    return lax.ppermute(a, "tp", where)


def routed_experts(low, high, both, gate, up, down):
    def run(own, *fetched, ready=(), tiles=4):
        return expert(own, fetched, ready, gate, up, down, tiles)

    def swap(*parts):
        return [shift(part, OTHER_CORE) for part in parts]

    below_low, above_high = shift(low, UP), shift(high, DOWN)
    other = shift(both, OTHER_CORE)
    below_high, above_low = shift(high, UP), shift(low, DOWN)
    own_low, own_high, own = run((low, high), other)
    far_low, far_high = shift(below_low, UP), shift(above_high, DOWN)
    near = (below_low, above_high)
    *first, others = run(near, *swap(*near), ready=(own,))
    first += swap(others)
    late = (below_high, above_low)
    *second, others = run(late, *swap(*late))
    second += swap(others)
    ends = (far_low, far_high)
    *far, others = run(ends, *swap(*ends), tiles=2)
    far += swap(others)
    rows = low.shape[0]
    pieces = ((0, EARLY), (EARLY, rows - EARLY))
    to_below, to_above = add_both(*first, ((0, rows),), skip=2 * rows)
    from_above_low, from_below_high = shift(to_below, DOWN), shift(to_above, UP)
    to_far = add_both(*far, pieces)
    from_below_low, from_above_high = [], []
    for k, window in enumerate(pieces):
        ups, downs = shift(to_far[k], UP), shift(to_far[2 + k], DOWN)
        ups = add(second[1], second[2], 1, ups, *window)
        downs = add(second[0], second[2], 0, downs, *window)
        from_below_low.append(shift(ups, UP))
        from_above_high.append(shift(downs, DOWN))
    return (
        (own_low, own_high),
        (first[2],),
        (*from_below_low, from_below_high),
        (from_above_low, *from_above_high),
    )


STATE = 136


def write_state(out_ref, total, state):
    high = total.astype(BF).astype(F32)
    row = lax.broadcasted_iota(jnp.int32, (8, state.shape[1]), 0)
    line = jnp.where(row == 0, high, jnp.where(row == 1, total - high, 0.0))
    message = jnp.concatenate([state, line], axis=0).astype(BF)
    for k in range(out_ref.shape[0]):
        out_ref[k] = message


def read_states(ref):
    size = ref.shape[2]
    states = [ref[k, :size, :].astype(F32) for k in range(ref.shape[0])]
    lines = [ref[k, size:, :].astype(F32) for k in range(ref.shape[0])]
    return [line[0:1, :] + line[1:2, :] for line in lines], states


def weighted(totals, states, end):
    result = jnp.zeros_like(states[0])
    between = jnp.zeros_like(totals[0])
    for k in reversed(range(len(states))):
        result = result + jnp.where(k < end, jnp.exp(between), 0.0) * states[k]
        between = between + jnp.where(k < end, totals[k], 0.0)
    return result, between


def rotate(ref, cos_ref, sin_ref):
    rows = ref[...].astype(F32)
    return rows * cos_ref[...] + pltpu.roll(rows, ref.shape[1] // 2, 1) * sin_ref[...]


def block_state_kernel(
    key_ref, value_ref, decay_ref, cos_ref, sin_ref, row_ref, column_ref, out_ref, ready
):
    ready()
    width = key_ref.shape[1]
    blocks = decay_ref.shape[1] // width
    decay = jnp.concatenate(
        [decay_ref[:, k * width : (k + 1) * width] for k in range(blocks)]
        + [jnp.zeros((-blocks % 8, width), F32)],
        axis=0,
    )
    blocks = decay.shape[0]
    high = decay.astype(BF).astype(F32)
    middle = (decay - high).astype(BF).astype(F32)
    words = jnp.concatenate([high, middle, decay - high - middle], axis=0).astype(BF)
    upper = onehot(
        lax.broadcasted_iota(jnp.int32, (width, width), 0)
        <= lax.broadcasted_iota(jnp.int32, (width, width), 1)
    )
    sums = dot(words, upper)
    sums = sums[:blocks] + sums[blocks : 2 * blocks] + sums[2 * blocks :]
    total = jnp.zeros((1, 1), F32)
    rows = []
    for k in range(row_ref.shape[1] // width):
        rows.append(sums[k : k + 1, :] + total)
        total = rows[-1][:, width - 1 :]
    row_ref[...] = jnp.concatenate(rows, axis=1)
    column = jnp.concatenate([jnp.broadcast_to(r, (width, width)).T for r in rows], axis=0)
    column_ref[...] = column
    rotated = rotate(key_ref, cos_ref, sin_ref).astype(BF)
    damped = (rotated.astype(F32) * jnp.exp(total - column)).astype(BF)
    state = lax.dot_general(
        damped, value_ref[...], (((0,), (0,)), ((), ())), preferred_element_type=F32
    )
    write_state(out_ref, total, state)


def chip_row_kernel(in_ref, index_ref, inside_ref, ahead_ref, out_ref):
    totals, states = read_states(in_ref)
    inside, ahead = weighted(totals, states, index_ref[...])
    inside_ref[...] = inside
    ahead_ref[...] = ahead
    state, total = weighted(totals, states, len(states))
    write_state(out_ref, total, state)


def within_kernel(
    query_ref, key_ref, value_ref, row_ref, column_ref, cos_ref, sin_ref, turned_ref, out_ref, rotated
):
    width = query_ref.shape[1]
    turned_ref[...] = (rotate(query_ref, cos_ref, sin_ref) * width**-0.5).astype(BF)
    rotated[...] = rotate(key_ref, cos_ref, sin_ref).astype(BF)
    step = 256

    def some_rows(k, carry):
        place = pl.ds(k * step, step)
        scores = lax.dot_general(
            turned_ref[place, :],
            rotated[...],
            (((1,), (1,)), ((), ())),
            preferred_element_type=F32,
        )
        i = lax.broadcasted_iota(jnp.int32, scores.shape, 0) + k * step
        causal = i >= lax.broadcasted_iota(jnp.int32, scores.shape, 1)
        spread = column_ref[place, 0:1] - row_ref[...]
        decays = jnp.where(causal, jnp.exp(jnp.where(causal, spread, 0.0)), 0.0)
        out_ref[place, :] = dot((scores * decays).astype(BF), value_ref[...])
        return carry

    lax.fori_loop(0, query_ref.shape[0] // step, some_rows, 0)


def mix_kernel(
    in_ref, index_ref, inside_ref, ahead_ref, turned_ref, within_ref, column_ref, gate_ref, gain_ref, out_ref, ready
):
    totals, states = read_states(in_ref)
    before, _ = weighted(totals, states, index_ref[...])
    carried = jnp.exp(ahead_ref[...]) * before + inside_ref[...]
    high = carried.astype(BF)
    low = (carried - high.astype(F32)).astype(BF)
    ready()
    turned = turned_ref[...]
    readout = dot(turned, high) + dot(turned, low)
    out = within_ref[...] + jnp.exp(column_ref[...]) * readout
    scale = lax.rsqrt(jnp.mean(out * out, axis=1, keepdims=True) + epsilon)
    gate = gate_ref[...].astype(F32)
    out_ref[...] = (out * scale * gain_ref[...] * jax.nn.silu(gate)).astype(BF)


def slot_indices(route_ids, experts):
    flat_ids = route_ids.reshape(-1)
    chosen = (flat_ids[:, None] == jnp.arange(experts, dtype=jnp.int32)[None, :]).astype(BF)
    place = jnp.arange(flat_ids.shape[0])
    before = dot((place[:, None] > place[None, :]).astype(BF), chosen)
    rank_in = jnp.sum(before * chosen.astype(F32), axis=1).astype(jnp.int32)
    return (flat_ids * SLOTS + rank_in).reshape(route_ids.shape)


def layer(
    residual,
    queries,
    key_rows,
    value_rows,
    gate_rows,
    log_decay,
    out_gain,
    out_weight,
    norm_gain,
    expert_gate,
    expert_up,
    expert_down,
    routes,
    route_weight,
):
    length, head_dim = queries.shape
    sp_count = lax.axis_size(SP)
    tp = lax.axis_index("tp")
    tp_count = lax.axis_size("tp")
    positions = (lax.axis_index(SP) * length + jnp.arange(length, dtype=jnp.int32)).astype(F32)
    column = jnp.arange(head_dim)
    half_dim = head_dim // 2
    inverse = rope_base ** (-(2 * (column % half_dim)).astype(F32) / head_dim)
    angles = positions[:, None] * inverse[None, :]
    cosine = jnp.cos(angles)
    sine = jnp.sin(angles) * jnp.where(column < half_dim, -1.0, 1.0)[None, :]
    shape = jax.ShapeDtypeStruct
    decay_row, decay_column, message = vmem_call(
        block_state_kernel,
        [
            shape((1, length), F32),
            shape((length, head_dim), F32),
            shape((lax.axis_size("sp_1"), STATE, head_dim), BF),
        ],
        late=(0, 1, 2),
    )(key_rows, value_rows, log_decay, cosine, sine)
    pieces = lax.all_to_all(message, "sp_1", 0, 0, tiled=True)
    rotated_queries, within = vmem_call(
        within_kernel,
        [shape((length, head_dim), BF), shape((length, head_dim), F32)],
        scratch_shapes=[pltpu.VMEM((length, head_dim), BF)],
        cost_estimate=pl.CostEstimate(
            flops=3 * length * length * head_dim,
            bytes_accessed=12 * length * head_dim,
            transcendentals=length * length,
        ),
    )(queries, key_rows, value_rows, decay_row, decay_column, cosine, sine)

    def index_line(axis):
        return jnp.full((1, head_dim), lax.axis_index(axis), jnp.int32)

    inside, ahead, message = vmem_call(
        chip_row_kernel,
        [
            shape((head_dim, head_dim), F32),
            shape((1, head_dim), F32),
            shape((lax.axis_size("sp_0"), STATE, head_dim), BF),
        ],
    )(pieces, index_line("sp_1"))
    pieces = lax.all_to_all(message, "sp_0", 0, 0, tiled=True)
    mixed = vmem_call(mix_kernel, shape((length, head_dim), BF), late=(4, 5, 7))(
        pieces,
        index_line("sp_0"),
        inside,
        ahead,
        rotated_queries,
        within,
        decay_column,
        gate_rows,
        out_gain[None],
    )

    weights = [
        out_weight, shift(out_weight, DOWN), shift(out_weight, ACROSS), shift(out_weight, UP)
    ]
    weights = weights + [shift(w, OTHER_CORE) for w in weights]

    row_count, model_width = residual.shape
    heads = lax.all_to_all(
        mixed.reshape(tp_count, row_count, head_dim), "tp", 0, 0, tiled=True
    )
    chip, core = tp // 2, tp % 2
    turned = lax.dynamic_slice_in_dim(jnp.concatenate([heads, heads]), 2 * chip, tp_count, 0)
    turned = turned.reshape(tp_count // 2, 2, row_count, head_dim)
    mine = jnp.where(core == 0, turned[:, 0], turned[:, 1])
    others = jnp.where(core == 0, turned[:, 1], turned[:, 0])

    slots = slot_indices(routes, sp_count)
    size = sp_count * SLOTS
    packed = shape((size, USED * BLOCK), BF)
    message = (sp_count, SLOTS, USED * BLOCK)
    turning = [pltpu.VMEM(packed.shape, BF)]
    hidden_res, tokens = vmem_call(
        project_and_pack_kernel,
        [shape((row_count, model_width), BF), packed],
        late=(10,),
        scratch_shapes=turning,
    )(mine, others, *weights, residual, norm_gain[None], slots.T)
    landed = lax.all_to_all(tokens.reshape(message), SP, 0, 0, tiled=True)
    half = shape((sp_count * USED // 2, model_width), BF)
    rows = vmem_call(
        unpack_rows_kernel, [half, half, shape((sp_count * USED, model_width), BF)]
    )(landed.reshape(packed.shape))
    route = shape((row_count, sp_count * USED), BF)
    high_weight, low_weight = vmem_call(route_rows_kernel, [route, route])(slots, route_weight)
    parts = routed_experts(*rows, expert_gate, expert_up, expert_down)
    counts = tuple(map(len, parts))
    repacked = vmem_call(
        lambda *refs: repack_rows_kernel(*refs, counts=counts), packed, scratch_shapes=turning
    )(*[ref for part in parts for ref in part])
    returned = lax.all_to_all(repacked.reshape(message), SP, 0, 0, tiled=True)
    return vmem_call(
        combine_kernel,
        shape(residual.shape, BF),
        scratch_shapes=[pltpu.VMEM((sp_count * USED, model_width), BF)],
    )(returned.reshape(packed.shape), hidden_res, high_weight, low_weight)


def solution(mesh):
    split = Mesh(mesh.devices.reshape(8, 4, mesh.shape["tp"]), ("sp_0", "sp_1", "tp"))
    in_specs = (
        P(SP_TP, None),
        P(SP, "tp"),
        P(SP, "tp"),
        P(SP, "tp"),
        P(SP, "tp"),
        P("tp", SP),
        P("tp"),
        P("tp", None),
        P(),
        P(SP, None, "tp"),
        P(SP, None, "tp"),
        P(SP, "tp", None),
        P(SP_TP, None),
        P(SP_TP, None),
    )
    out_specs = P(SP_TP, None)
    return jax.shard_map(layer, mesh=split, in_specs=in_specs, out_specs=out_specs, check_vma=False)
```

```python
import jax
import jax.numpy as jnp
from jax import lax
from jax.experimental import pallas as pl
from jax.experimental.pallas import tpu as pltpu
from jax.sharding import Mesh
from jax.sharding import PartitionSpec as P


SP = ("sp_0", "sp_1")
SP_TP = ("sp_0", "sp_1", "tp")


epsilon = 1e-06
rope_base = 10000.0
BF = jnp.bfloat16
F32 = jnp.float32

OTHER_CORE = [(i, i ^ 1) for i in range(8)]
UP = [(i, (i + 2) % 8) for i in range(8)]
DOWN = [(i, (i - 2) % 8) for i in range(8)]
ACROSS = [(i, (i + 4) % 8) for i in range(8)]

SLOTS = 8
USED = 7
UNIT = 16
BLOCK = 256
EARLY = 64


def dot(a, b):
    return jnp.dot(a, b, preferred_element_type=F32)


def whole(shape):
    return pl.BlockSpec(shape, lambda j: (0,) * len(shape))


def vmem_call(kernel, out_shape, late=(), scratch_shapes=(), **kwargs):
    def call(*args):
        args = [
            pltpu.with_memory_space_constraint(a, pltpu.HBM) if k in late else a
            for k, a in enumerate(args)
        ]
        count = len(args)
        outs = len(jax.tree.leaves(out_shape))
        buffers = [pltpu.VMEM(args[k].shape, args[k].dtype) for k in late]
        signals = [pltpu.SemaphoreType.DMA(())] * len(late)

        def body(*refs):
            ins = list(refs[:count])
            rest = refs[count : count + outs + len(scratch_shapes)]
            extra = refs[count + outs + len(scratch_shapes) :]
            copies = []
            for n, k in enumerate(late):
                copies.append(pltpu.make_async_copy(ins[k], extra[n], extra[len(late) + n]))
                copies[-1].start()
                ins[k] = extra[n]

            def ready():
                for copy in copies:
                    copy.wait()

            if late:
                kernel(*ins, *rest, ready=ready)
            else:
                kernel(*ins, *rest)

        return pl.pallas_call(
            body,
            in_specs=[
                pl.BlockSpec(memory_space=pltpu.HBM if k in late else pltpu.VMEM)
                for k in range(count)
            ],
            out_shape=out_shape,
            scratch_shapes=[*scratch_shapes, *buffers, *signals],
            compiler_params=pltpu.CompilerParams(vmem_limit_bytes=12 * 1024 * 1024),
            **kwargs,
        )(*args)

    return call


def onehot(mask):
    return jnp.where(mask, 1.0, 0.0).astype(BF)


def by_block(size):
    peers = size // SLOTS
    to = lax.broadcasted_iota(jnp.int32, (size, size), 0)
    source = lax.broadcasted_iota(jnp.int32, (size, size), 1)
    return onehot(source == (to & (peers - 1)) * SLOTS + to // peers)


def by_peer(size):
    peers = size // SLOTS
    to = lax.broadcasted_iota(jnp.int32, (size, size), 0)
    source = lax.broadcasted_iota(jnp.int32, (size, size), 1)
    return onehot(source == (to & 7) * peers + to // SLOTS)


def slot_of_row(shape, dim, peers):
    row = lax.broadcasted_iota(jnp.int32, shape, dim)
    return (row & (peers - 1)) * SLOTS + row // peers


def project_and_pack_kernel(*refs, ready):
    mine_ref, others_ref = refs[:2]
    weights = refs[2:10]
    residual_ref, gain_ref, slot_ref, hidden_ref, out_ref, turned = refs[10:]
    tokens, width = residual_ref.shape
    size = out_ref.shape[0]
    peers = size // SLOTS
    heads = [ref[k] for ref in (mine_ref, others_ref) for k in range(4)]
    squares = jnp.zeros((tokens, 1), F32)
    step = 512
    for start in range(0, width, step):
        columns = slice(start, start + step)
        projected = sum(dot(head, w[:, columns]) for head, w in zip(heads, weights))
        if start == 0:
            ready()
        hidden = (residual_ref[:, columns].astype(F32) + projected).astype(BF)
        hidden_ref[:, columns] = hidden
        hidden_f = hidden.astype(F32)
        squares = squares + jnp.sum(hidden_f * hidden_f, axis=1, keepdims=True)
    scale = lax.rsqrt(squares / width + epsilon)
    slot = slot_of_row((USED * peers, tokens), 0, peers)
    chosen = onehot((slot == slot_ref[0:1, :]) | (slot == slot_ref[1:2, :]))
    for i in range(SLOTS):
        columns = slice(i * BLOCK, (i + 1) * BLOCK)
        normed = hidden_ref[:, columns].astype(F32) * scale * gain_ref[:, columns]
        picked = dot(chosen, normed.astype(BF)).astype(BF)
        for c in range(USED):
            turned[i * peers : (i + 1) * peers, c * BLOCK : (c + 1) * BLOCK] = picked[
                c * peers : (c + 1) * peers, :
            ]
    out_ref[...] = dot(by_peer(size), turned[...]).astype(BF)


def units(refs):
    for ref in refs:
        for start in range(0, ref.shape[0], UNIT):
            yield ref, slice(start, start + UNIT)


def unpack(in_ref, *out_refs):
    size = in_ref.shape[0]
    peers = size // SLOTS
    order = by_block(size)
    places = list(units(out_refs))
    each = peers // UNIT
    for c in range(in_ref.shape[1] // BLOCK):
        rows = dot(order, in_ref[:, c * BLOCK : (c + 1) * BLOCK]).astype(BF)
        for k in range(each):
            ref, place = places[c * each + k]
            for i in range(SLOTS):
                start = i * peers + k * UNIT
                ref[place, i * BLOCK : (i + 1) * BLOCK] = rows[start : start + UNIT, :]


def by_unit(rows, body):
    def step(k, carry):
        body(pl.multiple_of(k * UNIT, UNIT))
        return carry

    lax.fori_loop(0, rows // UNIT, step, 0)


def copy_rows(out_ref, out_start, in_ref, in_start, rows):
    def body(start):
        out_ref[pl.ds(out_start + start, UNIT), :] = in_ref[pl.ds(in_start + start, UNIT), :]

    by_unit(rows, body)


def unpack_rows_kernel(in_ref, low_ref, high_ref, both_ref):
    unpack(in_ref, low_ref, high_ref)
    half = low_ref.shape[0]
    copy_rows(both_ref, 0, low_ref, 0, half)
    copy_rows(both_ref, half, high_ref, 0, half)


def repack_rows_kernel(*refs, counts):
    out_ref, turned = refs[-2:]
    size = out_ref.shape[0]
    peers = size // SLOTS
    each = peers // UNIT
    sources, start = [], 0
    for count in counts:
        sources.append(refs[start : start + count])
        start += count
    for u, parts in enumerate(zip(*map(units, sources))):
        total = sum(ref[place, :].astype(F32) for ref, place in parts).astype(BF)
        c, start = u // each, u % each * UNIT
        for i in range(SLOTS):
            turned[i * peers + start : i * peers + start + UNIT, c * BLOCK : (c + 1) * BLOCK] = (
                total[:, i * BLOCK : (i + 1) * BLOCK]
            )
    out_ref[...] = dot(by_peer(size), turned[...]).astype(BF)


def add_kernel(*refs, windows):
    outs = refs[-len(windows) :]
    for (own, core, more, own_first, core_first), out_ref in zip(windows, outs):

        def body(start):
            total = refs[own][pl.ds(own_first + start, UNIT), :].astype(F32)
            total = total + refs[core][pl.ds(core_first + start, UNIT), :].astype(F32)
            if more is not None:
                total = total + refs[more][pl.ds(start, UNIT), :].astype(F32)
            out_ref[pl.ds(start, UNIT), :] = total.astype(BF)

        by_unit(out_ref.shape[0], body)


def add(own, core, second, more, first, rows):
    windows = [(0, 1, 2, first, own.shape[0] * second + first)]
    return vmem_call(
        lambda *refs: add_kernel(*refs, windows=windows),
        [jax.ShapeDtypeStruct((rows, own.shape[1]), BF)],
    )(own, core, more)[0]


def add_both(a, b, core, pieces, skip=0):
    rows, width = a.shape
    windows = [
        (half, 2, None, first, skip + rows * half + first) for half in (0, 1) for first, _ in pieces
    ]
    return vmem_call(
        lambda *refs: add_kernel(*refs, windows=windows),
        [jax.ShapeDtypeStruct((count, width), BF) for _ in (0, 1) for _, count in pieces],
    )(a, b, core)


def route_rows_kernel(slot_ref, weight_ref, high_ref, low_ref):
    slot = slot_of_row(high_ref.shape, 1, high_ref.shape[1] // USED)
    weight = sum(
        jnp.where(slot == slot_ref[:, k : k + 1], weight_ref[:, k : k + 1], 0.0) for k in (0, 1)
    )
    high = weight.astype(BF)
    high_ref[...] = high
    low_ref[...] = (weight - high.astype(F32)).astype(BF)


def combine_kernel(rows_ref, hidden_ref, high_ref, low_ref, out_ref, rows):
    unpack(rows_ref, rows)
    for i in range(SLOTS):
        columns = slice(i * BLOCK, (i + 1) * BLOCK)
        block = rows[:, columns]
        got = dot(high_ref[...], block) + dot(low_ref[...], block)
        out_ref[:, columns] = (hidden_ref[:, columns].astype(F32) + got).astype(BF)


def expert_kernel(*refs, count, ready, tiles):
    parts = refs[:count]
    gate_ref, up_ref, down_ref = refs[count : count + 3]
    passed = refs[count + 3 : count + 3 + ready]
    outs = refs[count + 3 + ready : -2]
    rows, total = refs[-2:]
    step = pl.program_id(0)

    def starts(pieces):
        start = 0
        for piece in pieces:
            yield start
            start += piece.shape[0]

    @pl.when(step == 0)
    def _():
        for part, start in zip(parts, starts(parts)):
            copy_rows(rows, start, part, 0, part.shape[0])

    tile = rows.shape[0] // tiles
    last = step == pl.num_programs(0) - 1

    def one_tile(k, carry):
        place = pl.ds(k * tile, tile)
        x = rows[place, :]
        hidden = (jax.nn.silu(dot(x, gate_ref[0])) * dot(x, up_ref[0])).astype(BF)
        piece = dot(hidden, down_ref[0])

        @pl.when(step == 0)
        def _():
            total[place, :] = piece

        @pl.when(last)
        def _():
            rows[place, :] = (total[place, :] + piece).astype(BF)

        return carry

    lax.fori_loop(0, tiles, one_tile, 0)

    @pl.when(last)
    def _():
        ahead = 0
        for ref in passed:
            copy_rows(outs[-1], ahead, ref, 0, ref.shape[0])
            ahead += ref.shape[0]
        for out, start in zip(outs, starts(outs)):
            first = ahead if out is outs[-1] else 0
            copy_rows(out, first, rows, start, out.shape[0] - first)


def expert(own, fetched, ready, gate, up, down, tiles):
    parts = (*own, *fetched)
    count = len(parts)
    ahead = sum(part.shape[0] for part in ready)
    height = sum(part.shape[0] for part in parts)
    width = parts[0].shape[1]
    chunk = gate.shape[2] // 2
    outs = [part.shape for part in own] + [(ahead + height // 2, width)]

    return pl.pallas_call(
        lambda *refs: expert_kernel(*refs, count=count, ready=len(ready), tiles=tiles),
        grid=(2,),
        in_specs=[whole(part.shape) for part in parts]
        + [
            pl.BlockSpec((1, width, chunk), lambda j: (0, 0, j)),
            pl.BlockSpec((1, width, chunk), lambda j: (0, 0, j)),
            pl.BlockSpec((1, chunk, width), lambda j: (0, j, 0)),
        ]
        + [whole(part.shape) for part in ready],
        out_specs=[whole(out) for out in outs],
        out_shape=[jax.ShapeDtypeStruct(out, BF) for out in outs],
        scratch_shapes=[pltpu.VMEM((height, width), BF), pltpu.VMEM((height, width), F32)],
        compiler_params=pltpu.CompilerParams(
            dimension_semantics=("arbitrary",), vmem_limit_bytes=20 * 1024 * 1024
        ),
        cost_estimate=pl.CostEstimate(
            flops=6 * height * width * gate.shape[2],
            bytes_accessed=2 * (2 * height * width + 3 * width * gate.shape[2]),
            transcendentals=height * gate.shape[2],
        ),
    )(*parts, gate, up, down, *ready)


def shift(a, where):
    return lax.ppermute(a, "tp", where)


def routed_experts(low, high, both, gate, up, down):
    def run(own, *fetched, ready=(), tiles=4):
        return expert(own, fetched, ready, gate, up, down, tiles)

    def swap(*parts):
        return [shift(part, OTHER_CORE) for part in parts]

    below_low, above_high = shift(low, UP), shift(high, DOWN)
    other = shift(both, OTHER_CORE)
    below_high, above_low = shift(high, UP), shift(low, DOWN)
    own_low, own_high, own = run((low, high), other)
    far_low, far_high = shift(below_low, UP), shift(above_high, DOWN)
    near = (below_low, above_high)
    *first, others = run(near, *swap(*near), ready=(own,))
    first += swap(others)
    late = (below_high, above_low)
    *second, others = run(late, *swap(*late), tiles=2)
    second += swap(others)
    ends = (far_low, far_high)
    *far, others = run(ends, *swap(*ends), tiles=1)
    far += swap(others)
    rows = low.shape[0]
    pieces = ((0, EARLY), (EARLY, rows - EARLY))
    to_below, to_above = add_both(*first, ((0, rows),), skip=2 * rows)
    from_above_low, from_below_high = shift(to_below, DOWN), shift(to_above, UP)
    to_far = add_both(*far, pieces)
    from_below_low, from_above_high = [], []
    for k, window in enumerate(pieces):
        ups, downs = shift(to_far[k], UP), shift(to_far[2 + k], DOWN)
        ups = add(second[1], second[2], 1, ups, *window)
        downs = add(second[0], second[2], 0, downs, *window)
        from_below_low.append(shift(ups, UP))
        from_above_high.append(shift(downs, DOWN))
    return (
        (own_low, own_high),
        (first[2],),
        (*from_below_low, from_below_high),
        (from_above_low, *from_above_high),
    )


STEP = 32
STATE = 136


def write_state(out_ref, total, state):
    high = total.astype(BF).astype(F32)
    row = lax.broadcasted_iota(jnp.int32, (8, state.shape[1]), 0)
    line = jnp.where(row == 0, high, jnp.where(row == 1, total - high, 0.0))
    message = jnp.concatenate([state, line], axis=0).astype(BF)
    for k in range(out_ref.shape[0]):
        out_ref[k] = message


def read_states(ref):
    size = ref.shape[2]
    states = [ref[k, :size, :].astype(F32) for k in range(ref.shape[0])]
    lines = [ref[k, size:, :].astype(F32) for k in range(ref.shape[0])]
    return [line[0:1, :] + line[1:2, :] for line in lines], states


def weighted(totals, states, end):
    result = jnp.zeros_like(states[0])
    between = jnp.zeros_like(totals[0])
    for k in reversed(range(len(states))):
        result = result + jnp.where(k < end, jnp.exp(between), 0.0) * states[k]
        between = between + jnp.where(k < end, totals[k], 0.0)
    return result, between


def rotary(cos_ref, sin_ref):
    steps = cos_ref.shape[0] - STEP
    near_cos, near_sin = cos_ref[steps:, :], sin_ref[steps:, :]
    cosine, sine = [], []
    for k in range(steps):
        far_cos, far_sin = cos_ref[k : k + 1, :], sin_ref[k : k + 1, :]
        cosine.append(far_cos * near_cos - far_sin * near_sin)
        sine.append(far_sin * near_cos + far_cos * near_sin)
    return jnp.concatenate(cosine, axis=0), jnp.concatenate(sine, axis=0)


def rotate(ref, cosine, sine):
    rows = ref[...].astype(F32)
    return rows * cosine + pltpu.roll(rows, ref.shape[1] // 2, 1) * sine


def column_of(row_ref, width):
    rows = [row_ref[:, k : k + width] for k in range(0, row_ref.shape[1], width)]
    return jnp.concatenate([jnp.broadcast_to(r, (width, width)).T for r in rows], axis=0)


def block_state_kernel(
    key_ref, value_ref, decay_ref, cos_ref, sin_ref, row_ref, out_ref, ready
):
    cosine, sine = rotary(cos_ref, sin_ref)
    ready()
    width = key_ref.shape[1]
    blocks = decay_ref.shape[1] // width
    decay = jnp.concatenate(
        [decay_ref[:, k * width : (k + 1) * width] for k in range(blocks)]
        + [jnp.zeros((-blocks % 8, width), F32)],
        axis=0,
    )
    blocks = decay.shape[0]
    high = decay.astype(BF).astype(F32)
    middle = (decay - high).astype(BF).astype(F32)
    words = jnp.concatenate([high, middle, decay - high - middle], axis=0).astype(BF)
    upper = onehot(
        lax.broadcasted_iota(jnp.int32, (width, width), 0)
        <= lax.broadcasted_iota(jnp.int32, (width, width), 1)
    )
    sums = dot(words, upper)
    sums = sums[:blocks] + sums[blocks : 2 * blocks] + sums[2 * blocks :]
    total = jnp.zeros((1, 1), F32)
    rows = []
    for k in range(row_ref.shape[1] // width):
        rows.append(sums[k : k + 1, :] + total)
        total = rows[-1][:, width - 1 :]
    row_ref[...] = jnp.concatenate(rows, axis=1)
    column = column_of(row_ref, width)
    rotated = rotate(key_ref, cosine, sine).astype(BF)
    damped = (rotated.astype(F32) * jnp.exp(total - column)).astype(BF)
    state = lax.dot_general(
        damped, value_ref[...], (((0,), (0,)), ((), ())), preferred_element_type=F32
    )
    write_state(out_ref, total, state)


def chip_row_kernel(in_ref, index_ref, inside_ref, ahead_ref, out_ref):
    totals, states = read_states(in_ref)
    inside, ahead = weighted(totals, states, index_ref[...])
    inside_ref[...] = inside
    ahead_ref[...] = ahead
    state, total = weighted(totals, states, len(states))
    write_state(out_ref, total, state)


def within_kernel(
    query_ref, key_ref, value_ref, row_ref, cos_ref, sin_ref, turned_ref, out_ref, rotated, column
):
    width = query_ref.shape[1]
    cosine, sine = rotary(cos_ref, sin_ref)
    turned_ref[...] = (rotate(query_ref, cosine, sine) * width**-0.5).astype(BF)
    rotated[...] = rotate(key_ref, cosine, sine).astype(BF)
    column[...] = column_of(row_ref, width)
    step = 256

    def some_rows(k, carry):
        place = pl.ds(k * step, step)
        scores = lax.dot_general(
            turned_ref[place, :],
            rotated[...],
            (((1,), (1,)), ((), ())),
            preferred_element_type=F32,
        )
        i = lax.broadcasted_iota(jnp.int32, scores.shape, 0) + k * step
        causal = i >= lax.broadcasted_iota(jnp.int32, scores.shape, 1)
        spread = column[place, 0:1] - row_ref[...]
        decays = jnp.where(causal, jnp.exp(jnp.where(causal, spread, 0.0)), 0.0)
        out_ref[place, :] = dot((scores * decays).astype(BF), value_ref[...])
        return carry

    lax.fori_loop(0, query_ref.shape[0] // step, some_rows, 0)


def mix_kernel(
    in_ref, index_ref, inside_ref, ahead_ref, turned_ref, within_ref, row_ref, gate_ref, gain_ref, out_ref, ready
):
    totals, states = read_states(in_ref)
    before, _ = weighted(totals, states, index_ref[...])
    carried = jnp.exp(ahead_ref[...]) * before + inside_ref[...]
    high = carried.astype(BF)
    low = (carried - high.astype(F32)).astype(BF)
    decay = jnp.exp(column_of(row_ref, turned_ref.shape[1]))
    ready()
    turned = turned_ref[...]
    readout = dot(turned, high) + dot(turned, low)
    out = within_ref[...] + decay * readout
    scale = lax.rsqrt(jnp.mean(out * out, axis=1, keepdims=True) + epsilon)
    gate = gate_ref[...].astype(F32)
    out_ref[...] = (out * scale * gain_ref[...] * jax.nn.silu(gate)).astype(BF)


def slot_indices(route_ids, experts):
    flat_ids = route_ids.reshape(-1)
    chosen = (flat_ids[:, None] == jnp.arange(experts, dtype=jnp.int32)[None, :]).astype(BF)
    place = jnp.arange(flat_ids.shape[0])
    before = dot((place[:, None] > place[None, :]).astype(BF), chosen)
    rank_in = jnp.sum(before * chosen.astype(F32), axis=1).astype(jnp.int32)
    return (flat_ids * SLOTS + rank_in).reshape(route_ids.shape)


def layer(
    residual,
    queries,
    key_rows,
    value_rows,
    gate_rows,
    log_decay,
    out_gain,
    out_weight,
    norm_gain,
    expert_gate,
    expert_up,
    expert_down,
    routes,
    route_weight,
):
    length, head_dim = queries.shape
    sp_count = lax.axis_size(SP)
    tp = lax.axis_index("tp")
    tp_count = lax.axis_size("tp")
    start = lax.axis_index(SP) * length
    positions = jnp.concatenate(
        [start + jnp.arange(0, length, STEP, dtype=jnp.int32), jnp.arange(STEP, dtype=jnp.int32)]
    ).astype(F32)
    column = jnp.arange(head_dim)
    half_dim = head_dim // 2
    inverse = rope_base ** (-(2 * (column % half_dim)).astype(F32) / head_dim)
    angles = positions[:, None] * inverse[None, :]
    cosine = jnp.cos(angles)
    sine = jnp.sin(angles) * jnp.where(column < half_dim, -1.0, 1.0)[None, :]
    shape = jax.ShapeDtypeStruct
    decay_row, message = vmem_call(
        block_state_kernel,
        [
            shape((1, length), F32),
            shape((lax.axis_size("sp_1"), STATE, head_dim), BF),
        ],
        late=(0, 1, 2),
    )(key_rows, value_rows, log_decay, cosine, sine)
    pieces = lax.all_to_all(message, "sp_1", 0, 0, tiled=True)
    rotated_queries, within = vmem_call(
        within_kernel,
        [shape((length, head_dim), BF), shape((length, head_dim), F32)],
        scratch_shapes=[pltpu.VMEM((length, head_dim), BF), pltpu.VMEM((length, head_dim), F32)],
        cost_estimate=pl.CostEstimate(
            flops=3 * length * length * head_dim,
            bytes_accessed=12 * length * head_dim,
            transcendentals=length * length,
        ),
    )(queries, key_rows, value_rows, decay_row, cosine, sine)

    def index_line(axis):
        return jnp.full((1, head_dim), lax.axis_index(axis), jnp.int32)

    inside, ahead, message = vmem_call(
        chip_row_kernel,
        [
            shape((head_dim, head_dim), F32),
            shape((1, head_dim), F32),
            shape((lax.axis_size("sp_0"), STATE, head_dim), BF),
        ],
    )(pieces, index_line("sp_1"))
    pieces = lax.all_to_all(message, "sp_0", 0, 0, tiled=True)
    mixed = vmem_call(mix_kernel, shape((length, head_dim), BF), late=(4, 5, 7))(
        pieces,
        index_line("sp_0"),
        inside,
        ahead,
        rotated_queries,
        within,
        decay_row,
        gate_rows,
        out_gain[None],
    )

    weights = [
        out_weight, shift(out_weight, DOWN), shift(out_weight, ACROSS), shift(out_weight, UP)
    ]
    weights = weights + [shift(w, OTHER_CORE) for w in weights]

    row_count, model_width = residual.shape
    heads = lax.all_to_all(
        mixed.reshape(tp_count, row_count, head_dim), "tp", 0, 0, tiled=True
    )
    chip, core = tp // 2, tp % 2
    turned = lax.dynamic_slice_in_dim(jnp.concatenate([heads, heads]), 2 * chip, tp_count, 0)
    turned = turned.reshape(tp_count // 2, 2, row_count, head_dim)
    mine = jnp.where(core == 0, turned[:, 0], turned[:, 1])
    others = jnp.where(core == 0, turned[:, 1], turned[:, 0])

    slots = slot_indices(routes, sp_count)
    size = sp_count * SLOTS
    packed = shape((size, USED * BLOCK), BF)
    message = (sp_count, SLOTS, USED * BLOCK)
    turning = [pltpu.VMEM(packed.shape, BF)]
    hidden_res, tokens = vmem_call(
        project_and_pack_kernel,
        [shape((row_count, model_width), BF), packed],
        late=(10,),
        scratch_shapes=turning,
    )(mine, others, *weights, residual, norm_gain[None], slots.T)
    landed = lax.all_to_all(tokens.reshape(message), SP, 0, 0, tiled=True)
    half = shape((sp_count * USED // 2, model_width), BF)
    rows = vmem_call(
        unpack_rows_kernel, [half, half, shape((sp_count * USED, model_width), BF)]
    )(landed.reshape(packed.shape))
    route = shape((row_count, sp_count * USED), BF)
    high_weight, low_weight = vmem_call(route_rows_kernel, [route, route])(slots, route_weight)
    parts = routed_experts(*rows, expert_gate, expert_up, expert_down)
    counts = tuple(map(len, parts))
    repacked = vmem_call(
        lambda *refs: repack_rows_kernel(*refs, counts=counts), packed, scratch_shapes=turning
    )(*[ref for part in parts for ref in part])
    returned = lax.all_to_all(repacked.reshape(message), SP, 0, 0, tiled=True)
    return vmem_call(
        combine_kernel,
        shape(residual.shape, BF),
        scratch_shapes=[pltpu.VMEM((sp_count * USED, model_width), BF)],
    )(returned.reshape(packed.shape), hidden_res, high_weight, low_weight)


def solution(mesh):
    split = Mesh(mesh.devices.reshape(8, 4, mesh.shape["tp"]), ("sp_0", "sp_1", "tp"))
    in_specs = (
        P(SP_TP, None),
        P(SP, "tp"),
        P(SP, "tp"),
        P(SP, "tp"),
        P(SP, "tp"),
        P("tp", SP),
        P("tp"),
        P("tp", None),
        P(),
        P(SP, None, "tp"),
        P(SP, None, "tp"),
        P(SP, "tp", None),
        P(SP_TP, None),
        P(SP_TP, None),
    )
    out_specs = P(SP_TP, None)
    return jax.shard_map(layer, mesh=split, in_specs=in_specs, out_specs=out_specs, check_vma=False)
```
